32 devices in a mesh: sp: 16 (over z, y, x), tp: 2 (over core).
Axes of the slice: x: 2, y: 2, z: 4, core: 2. Of those that a mesh axis runs over, the one named last changes fastest.
Arguments:
- tokens: bfloat16 [6144, 4096], P(('sp', 'tp')), may hold values from -6 to 6
- norm_gain: float32 [4096], replicated, may hold values from 0.1 to 1.9
- conv_val_w: bfloat16 [4096, 1024], P('sp', 'tp'), may hold values from -0.09375 to 0.09375
- conv_gate_w: bfloat16 [4096, 1024], P('sp', 'tp'), may hold values from -0.09375 to 0.09375
- rec_gate_w: bfloat16 [4096, 1536], P('sp', 'tp'), may hold values from -0.09375 to 0.09375
- rec_in_w: bfloat16 [4096, 1536], P('sp', 'tp'), may hold values from -0.09375 to 0.09375
- conv_taps: bfloat16 [31, 1024], P(None, 'tp'), may hold values from -3 to 3
- conv_bias: float32 [1024], P('tp'), may hold values from 1 to 15
- conv_gain: float32 [1024], P('tp'), may hold values from 0.1 to 1.9
- short_taps: bfloat16 [4, 1536], P(None, 'tp'), may hold values from -3 to 3
- decay_map: bfloat16 [24, 64, 64], P('tp'), may hold values from -0.75 to 0.75
- input_map: bfloat16 [24, 64, 64], P('tp'), may hold values from -0.75 to 0.75
- decay_base: float32 [1536], P('tp'), may hold values from 3.5 to 17
- decay_jump: float32 [6144, 1536], P('sp', 'tp'), may hold values from -1.5 to 0
- out_conv_w: bfloat16 [1024, 4096], P('tp', 'sp'), may hold values from -0.125 to 0.125
- out_rec_w: bfloat16 [1536, 4096], P('tp', 'sp'), may hold values from -0.125 to 0.125
Outputs:
- mixed: bfloat16 [6144, 4096], P(('sp', 'tp'))
The draws below stay inside these ranges and needn't reach their ends.
All inputs are finite; a program needn't handle non-finite values.
Results may differ from the reference program's by a relative error of at most 0.015.
Values may be sent and summed in bfloat16 or wider, within the bound.
A program may use at most 128 MiB of HBM per device.

```python
import math
import jax
import jax.numpy as jnp
from jax import lax

D = 4096
HEAD_SIZE = 64
LRU_HEADS = 24
TAPS = 31
SHORT_TAPS = 4
CONV_WIDTH = 1024
LRU_WIDTH = 1536
TOKENS = 6144
N_TP = 2


def draw_conv_taps(key, part):
    key_base, key_jitter = jax.random.split(jax.random.fold_in(key, 31))
    channel = jnp.arange(CONV_WIDTH, dtype=jnp.float32) / CONV_WIDTH
    jitter = jnp.exp(jax.random.uniform(key_jitter, (CONV_WIDTH,), jnp.float32, math.log(0.8), math.log(1.25)))
    base = jnp.clip(jax.random.normal(key_base, (TAPS, CONV_WIDTH), jnp.float32), -4.0, 4.0)
    rising = jnp.exp(math.log(3.0) * channel)
    return (base * (rising * jitter)[None, :] * (1.0 / math.sqrt(TAPS))).astype(jnp.bfloat16)


def draw_conv_bias(key, part):
    key_jitter = jax.random.fold_in(key, 37)
    channel = jnp.arange(CONV_WIDTH, dtype=jnp.float32) / CONV_WIDTH
    jitter = jnp.exp(jax.random.uniform(key_jitter, (CONV_WIDTH,), jnp.float32, math.log(0.8), math.log(1.25)))
    rising = jnp.exp(math.log(4.0) * channel)
    return 1.5 * rising * jitter


def draw_decay_base(key, part):
    key_kind, key_slow, key_fast = jax.random.split(jax.random.fold_in(key, 29), 3)
    keep_share = 0.5
    slow = jax.random.uniform(key_kind, (LRU_WIDTH,), jnp.float32) < keep_share
    slow_rate = jnp.exp(jax.random.uniform(key_slow, (LRU_WIDTH,), jnp.float32, math.log(0.01), math.log(0.05))) / TOKENS
    fast_rate = jnp.exp(jax.random.uniform(key_fast, (LRU_WIDTH,), jnp.float32, math.log(0.0075), math.log(0.025)))
    rate = jnp.where(slow, slow_rate, fast_rate)
    return -jnp.log(jnp.expm1(rate))


def draw_decay_jump(key, part):
    key_leak, key_where, key_drop = jax.random.split(jax.random.fold_in(key, 23), 3)
    blocks = (TOKENS + 63) // 64
    lowest, highest = (0.05, 0.5)
    leak = jnp.exp(jax.random.uniform(key_leak, (blocks,), jnp.float32, math.log(lowest), math.log(highest))) / TOKENS
    position_leak = jnp.repeat(leak, 64)[:TOKENS]
    places = jax.random.randint(key_where, (2,), 0, TOKENS)
    hits = (jnp.arange(TOKENS)[:, None] == places[None, :]).astype(jnp.float32)
    drops = jnp.log1p(-jax.random.uniform(key_drop, (2, LRU_WIDTH), jnp.float32, 0.2, 0.5))
    return jnp.dot(hits, drops, precision=lax.Precision.HIGHEST) - position_leak[:, None]


def block_levels(stream_key, shape, pieces, low, high):
    level = 1.0
    for axis_at, blocks in pieces:
        heights = jax.random.uniform(jax.random.fold_in(jax.random.fold_in(stream_key, 6), axis_at), (blocks,), jnp.float32, low / len(pieces), high / len(pieces))
        level = level * jnp.repeat(jnp.exp(heights), shape[axis_at] // blocks).reshape((-1,) + (1,) * (len(shape) - 1 - axis_at))
    return level


def gaussian(key, shape, width, most, pieces=(), kind=jnp.bfloat16):
    level = block_levels(key, shape, pieces, -0.22, 0.18) if pieces else 1.0
    drawn = jax.random.normal(key, shape, jnp.float32) * width * level
    return jnp.minimum(jnp.maximum(drawn, -most), most).astype(kind)


def setup_inputs(seed: int = 0) -> dict:
    key_list = jax.random.split(jax.random.key(seed), 17)
    return {
        "tokens": gaussian(key_list[0], (TOKENS, D), 1.0, 6.0, ((0, 32),)),
        "norm_gain": jnp.clip(1.0 + 0.18 * jax.random.normal(key_list[1], (D,), jnp.float32), 0.1, 1.9),
        "conv_val_w": gaussian(key_list[2], (D, CONV_WIDTH), D ** -0.5, 0.09375, ((0, 16), (1, 2))),
        "conv_gate_w": gaussian(key_list[3], (D, CONV_WIDTH), D ** -0.5, 0.09375, ((0, 16), (1, 2))),
        "rec_gate_w": gaussian(key_list[4], (D, LRU_WIDTH), D ** -0.5, 0.09375, ((0, 16), (1, 2))),
        "rec_in_w": gaussian(key_list[5], (D, LRU_WIDTH), D ** -0.5, 0.09375, ((0, 16), (1, 2))),
        "conv_taps": draw_conv_taps(jax.random.fold_in(key_list[16], 71), 0),
        "conv_bias": draw_conv_bias(jax.random.fold_in(key_list[16], 71), 0),
        "conv_gain": jnp.clip(1.0 + 0.18 * jax.random.normal(key_list[8], (CONV_WIDTH,), jnp.float32), 0.1, 1.9),
        "short_taps": gaussian(key_list[9], (SHORT_TAPS, LRU_WIDTH), SHORT_TAPS ** -0.5, 3.0, ((1, 2),)),
        "decay_map": gaussian(key_list[10], (LRU_HEADS, HEAD_SIZE, HEAD_SIZE), HEAD_SIZE ** -0.5, 0.75, ((0, 2),)),
        "input_map": gaussian(key_list[11], (LRU_HEADS, HEAD_SIZE, HEAD_SIZE), HEAD_SIZE ** -0.5, 0.75, ((0, 2),)),
        "decay_base": draw_decay_base(jax.random.fold_in(key_list[16], 71), 0),
        "decay_jump": draw_decay_jump(jax.random.fold_in(key_list[16], 71), 0),
        "out_conv_w": gaussian(key_list[14], (CONV_WIDTH, D), (CONV_WIDTH + LRU_WIDTH) ** -0.5, 0.125, ((0, 2), (1, 16))),
        "out_rec_w": gaussian(key_list[15], (LRU_WIDTH, D), (CONV_WIDTH + LRU_WIDTH) ** -0.5, 0.125, ((0, 2), (1, 16))),
    }


RATE_SCALE = 8.0

def norm_rows(values, gain):
    widened = values.astype(jnp.float32)
    inverse = lax.rsqrt(lax.optimization_barrier(jnp.mean(widened * widened, axis=-1, keepdims=True)) + 1e-06)
    return (widened * inverse * gain).astype(jnp.bfloat16)

def causal_filter(signal, weights):
    lags = weights.shape[0]
    length = signal.shape[0]
    padded = jnp.pad(signal, ((lags - 1, 0), (0, 0)))
    result = jnp.zeros_like(signal)
    for lag_index in range(lags):
        result = result + weights[lag_index][None, :] * padded[lag_index:lag_index + length]
    return result

def chain_step(earlier, latter):
    return (earlier[0] * latter[0], latter[0] * earlier[1] + latter[1])

def reference(tokens, norm_gain, conv_val_w, conv_gate_w, rec_gate_w, rec_in_w, conv_taps, conv_bias, conv_gain, short_taps, decay_map, input_map, decay_base, decay_jump, out_conv_w, out_rec_w):
    normed = norm_rows(tokens, norm_gain)
    conv_val = jnp.dot(normed, conv_val_w, preferred_element_type=jnp.float32).astype(jnp.bfloat16)
    conv_gate = jnp.dot(normed, conv_gate_w, preferred_element_type=jnp.float32).astype(jnp.bfloat16)
    rec_gate = jnp.dot(normed, rec_gate_w, preferred_element_type=jnp.float32).astype(jnp.bfloat16)
    rec_in = jnp.dot(normed, rec_in_w, preferred_element_type=jnp.float32).astype(jnp.bfloat16)
    glu = (conv_val.astype(jnp.float32) * jax.nn.sigmoid(conv_gate.astype(jnp.float32))).astype(jnp.bfloat16)
    filtered = causal_filter(glu.astype(jnp.float32), conv_taps.astype(jnp.float32)) + conv_bias[None, :]
    centered = filtered - lax.optimization_barrier(jnp.mean(filtered, axis=1, keepdims=True))
    spread = lax.optimization_barrier(jnp.mean(centered * centered, axis=1, keepdims=True))
    conv_out = jax.nn.silu(centered * lax.rsqrt(spread + 1e-05) * conv_gain).astype(jnp.bfloat16)
    smoothed = causal_filter(rec_in.astype(jnp.float32), short_taps.astype(jnp.float32)).astype(jnp.bfloat16)
    grouped = smoothed.astype(jnp.float32).reshape(TOKENS, LRU_HEADS, HEAD_SIZE)
    retain = jax.nn.sigmoid(jnp.einsum('thi,hio->tho', grouped, decay_map.astype(jnp.float32)).reshape(TOKENS, LRU_WIDTH))
    admit = jax.nn.sigmoid(jnp.einsum('thi,hio->tho', grouped, input_map.astype(jnp.float32)).reshape(TOKENS, LRU_WIDTH))
    log_decay = -RATE_SCALE * retain * jax.nn.softplus(-decay_base)[None, :] + decay_jump
    decay = jnp.exp(log_decay)
    inflow = jnp.sqrt(-jnp.expm1(2.0 * log_decay)) * admit * smoothed.astype(jnp.float32)
    products, state = lax.associative_scan(chain_step, (decay, inflow), axis=0)
    rec_out = (jax.nn.gelu(rec_gate.astype(jnp.float32)) * state).astype(jnp.bfloat16)
    conv_block = CONV_WIDTH // N_TP
    rec_block = LRU_WIDTH // N_TP
    mixed = jnp.zeros((TOKENS, D), jnp.float32)
    for block_index in range(N_TP):
        conv_cols = slice(block_index * conv_block, (block_index + 1) * conv_block)
        rec_cols = slice(block_index * rec_block, (block_index + 1) * rec_block)
        term = jnp.dot(conv_out[:, conv_cols], out_conv_w[conv_cols], preferred_element_type=jnp.float32)
        term = term + jnp.dot(rec_out[:, rec_cols], out_rec_w[rec_cols], preferred_element_type=jnp.float32)
        mixed = mixed + lax.optimization_barrier(term.astype(jnp.bfloat16)).astype(jnp.float32)
    return mixed.astype(jnp.bfloat16)
```

```python
import functools

import jax
import jax.numpy as jnp
from jax import lax
from jax.experimental import pallas as pl
from jax.experimental.pallas import tpu as pltpu
from jax.sharding import PartitionSpec as P

CONV_WIDTH = 1024


RATE_SCALE = 8.0


def passed_along(value, axis, by):
    count = lax.axis_size(axis)
    pairs = [(i, i + by) for i in range(count) if 0 <= i + by < count]
    return lax.ppermute(value, axis, pairs)


def prefix(part, axis, combine, identity):
    place = lax.axis_index(axis)
    gathered = jax.tree.map(lambda a: lax.all_gather(a, axis), part)
    state = jax.tree.map(lambda a, e: jnp.zeros_like(a) + jnp.asarray(e, a.dtype), part, identity)

    def one(step, state):
        return combine(
            state, jax.tree.map(lambda a: lax.dynamic_index_in_dim(a, step, 0, False), gathered)
        )

    return lax.fori_loop(0, place, one, state)


def norm_rows(values, gain):
    widened = values.astype(jnp.float32)
    inverse = lax.rsqrt(jnp.mean(widened * widened, axis=-1, keepdims=True) + 1e-06)
    return (widened * inverse * gain).astype(jnp.bfloat16)


def causal_window(edge, current, weights):
    extended = jnp.concatenate([edge, current], axis=0).astype(jnp.float32)
    taps_wide = weights.astype(jnp.float32)
    length = current.shape[0]
    result = jnp.zeros((length, current.shape[1]), jnp.float32)
    for lag_index in range(weights.shape[0]):
        result = result + taps_wide[lag_index][None, :] * extended[lag_index : lag_index + length]
    return result


def chain_step(earlier, latter):
    return (earlier[0] * latter[0], latter[0] * earlier[1] + latter[1])


def glu_of(conv_val, conv_gate):
    return (conv_val.astype(jnp.float32) * jax.nn.sigmoid(conv_gate.astype(jnp.float32))).astype(
        jnp.bfloat16
    )


def shards(
    tokens,
    norm_gain,
    conv_val_w,
    conv_gate_w,
    rec_gate_w,
    rec_in_w,
    conv_taps,
    conv_bias,
    conv_gain,
    short_taps,
    decay_map,
    input_map,
    decay_base,
    decay_jump,
    out_conv_w,
    out_rec_w,
):
    rec_cols = rec_in_w.shape[1]
    conv_lags = conv_taps.shape[0] - 1
    short_lags = short_taps.shape[0] - 1
    normed = norm_rows(tokens, norm_gain)
    val_full, gate_full = (
        lax.all_gather(conv_val_w, "sp", axis=0, tiled=True),
        lax.all_gather(conv_gate_w, "sp", axis=0, tiled=True),
    )
    all_rows = lax.all_gather(normed, "tp", axis=0, tiled=True)
    conv_val = jnp.dot(all_rows, val_full, preferred_element_type=jnp.float32).astype(jnp.bfloat16)
    conv_gate = jnp.dot(all_rows, gate_full, preferred_element_type=jnp.float32).astype(
        jnp.bfloat16
    )
    glu = glu_of(conv_val, conv_gate)
    conv_edge = passed_along(glu[-conv_lags:], "sp", 1)
    rgate_full, rin_full = (
        lax.all_gather(rec_gate_w, "sp", axis=0, tiled=True),
        lax.all_gather(rec_in_w, "sp", axis=0, tiled=True),
    )
    rec_gate = jnp.dot(all_rows, rgate_full, preferred_element_type=jnp.float32).astype(
        jnp.bfloat16
    )
    rec_in = jnp.dot(all_rows, rin_full, preferred_element_type=jnp.float32).astype(jnp.bfloat16)
    rec_edge = passed_along(rec_in[-short_lags:], "sp", 1)
    filtered = causal_window(conv_edge, glu, conv_taps) + conv_bias[None, :]
    row_total = lax.psum(jnp.sum(filtered, axis=1), "tp")
    centered = filtered - (row_total / CONV_WIDTH)[:, None]
    spread = lax.psum(jnp.sum(centered * centered, axis=1), "tp") / CONV_WIDTH
    conv_out = jax.nn.silu(centered * lax.rsqrt(spread + 1e-05)[:, None] * conv_gain).astype(
        jnp.bfloat16
    )
    smoothed = causal_window(rec_edge, rec_in, short_taps).astype(jnp.bfloat16)
    length = smoothed.shape[0]
    grouped = smoothed.reshape(length, decay_map.shape[0], decay_map.shape[1])
    retain = jax.nn.sigmoid(
        jnp.einsum("thi,hio->tho", grouped, decay_map, preferred_element_type=jnp.float32).reshape(
            length, rec_cols
        )
    )
    admit = jax.nn.sigmoid(
        jnp.einsum("thi,hio->tho", grouped, input_map, preferred_element_type=jnp.float32).reshape(
            length, rec_cols
        )
    )
    log_decay = -RATE_SCALE * retain * jax.nn.softplus(-decay_base)[None, :] + decay_jump
    decay = jnp.exp(log_decay)
    inflow = jnp.sqrt(-jnp.expm1(2.0 * log_decay)) * admit * smoothed.astype(jnp.float32)
    products, local_state = lax.associative_scan(chain_step, (decay, inflow), axis=0)
    entering = prefix(
        (products[-1], local_state[-1]),
        "sp",
        chain_step,
        (jnp.ones((rec_cols,), jnp.float32), jnp.zeros((rec_cols,), jnp.float32)),
    )
    state = local_state + products * entering[1][None, :]
    rec_out = (jax.nn.gelu(rec_gate.astype(jnp.float32)) * state).astype(jnp.bfloat16)
    conv_full, rec_full = (
        lax.all_gather(out_conv_w, "sp", axis=1, tiled=True),
        lax.all_gather(out_rec_w, "sp", axis=1, tiled=True),
    )
    return lax.psum_scatter(
        (
            jnp.dot(conv_out, conv_full, preferred_element_type=jnp.float32)
            + jnp.dot(rec_out, rec_full, preferred_element_type=jnp.float32)
        ).astype(jnp.bfloat16),
        "tp",
        scatter_dimension=0,
        tiled=True,
    )


MESH = pl.DeviceIdType.MESH
ANY = pl.BlockSpec(memory_space=pl.ANY)
VMEM = pl.BlockSpec(memory_space=pltpu.VMEM)
SEGMENTS = 8


class Spot:
    def __init__(self, planes):
        self.s, self.c = lax.axis_index("sp"), lax.axis_index("tp")
        self.z, self.q = self.s // 4, self.s % 4
        self.qx = self.q + 1 - 2 * (self.q % 2)
        self.qy = (self.q + 2) % 4
        self.qd = 3 - self.q
        self.has_up, self.has_down = self.z < planes - 1, self.z > 0
        self.up, self.down = self.at(self.s + 4, self.c), self.at(self.s - 4, self.c)
        self.partner = self.at(self.s, 1 - self.c)

    def at(self, s, c):
        return {"sp": s, "tp": c}

    def mate(self, q):
        return self.at(self.z * 4 + q, self.c)


class Mail:
    def __init__(self, send_sem):
        self.send_sem, self.count, self.open = send_sem, 0, []

    def send(self, src, dst, recv, device, when=None):
        copy = pltpu.make_async_remote_copy(
            src_ref=src, dst_ref=dst, send_sem=self.send_sem.at[self.count],
            recv_sem=recv, device_id=device, device_id_type=MESH,
        )
        self.count += 1
        self.open.append((copy.wait_send, when))
        if when is None:
            copy.start()
        else:
            pl.when(when)(copy.start)

    def local(self, src, dst):
        copy = pltpu.make_async_copy(src, dst, self.send_sem.at[self.count])
        self.count += 1
        copy.start()
        self.open.append((copy.wait, None))

    def arrived(self, dst, recv, device):
        pltpu.make_async_remote_copy(
            src_ref=dst, dst_ref=dst, send_sem=self.send_sem.at[0],
            recv_sem=recv, device_id=device, device_id_type=MESH,
        ).wait_recv()

    def finish(self):
        for wait, when in self.open:
            if when is None:
                wait()
            else:
                pl.when(when)(wait)


def greet(me, devices, line):
    barrier = pltpu.get_barrier_semaphore()
    for device in devices:
        pl.semaphore_signal(barrier, inc=1, device_id=device, device_id_type=MESH)
    amount = len(devices)
    if line:
        for has, device in ((me.has_up, me.up), (me.has_down, me.down)):
            @pl.when(has)
            def _():
                pl.semaphore_signal(barrier, inc=1, device_id=device, device_id_type=MESH)
        amount = amount + me.has_up.astype(jnp.int32) + me.has_down.astype(jnp.int32)
    pl.semaphore_wait(barrier, amount)


class PlaneGather:
    def __init__(self, me, mail, own, slot, recv, recv_pair):
        self.me, self.mail, self.own, self.slot = me, mail, own, slot
        self.recv, self.recv_pair = recv, recv_pair

    def start(self):
        me, mail = self.me, self.mail
        for h in (0, 1):
            for q, half in ((me.qx, h), (me.qy, 1 - h)):
                mail.send(self.own(half), self.slot(me.q, me.c, half), self.recv.at[me.q, half], me.mate(q))
        for half in (0, 1):
            mail.send(self.own(half), self.slot(me.q, me.c, half), self.recv_pair.at[me.q, half], me.partner)

    def took(self, q, half):
        me, mail = self.me, self.mail
        here = self.slot(q, me.c, half)
        mail.arrived(here, self.recv.at[q, half], me.partner)
        return here

    def share(self, q, half, here):
        self.mail.send(here, here, self.recv_pair.at[q, half], self.me.partner)

    def first(self):
        me = self.me
        for q, half, to in ((me.qx, 0, me.qy), (me.qy, 1, me.qx)):
            here = self.took(q, half)
            self.mail.send(here, here, self.recv.at[q, half], me.mate(to))
            self.share(q, half, here)

    def second(self):
        for q, half in ((self.me.qx, 1), (self.me.qy, 0)):
            self.share(q, half, self.took(q, half))

    def third(self):
        for half in (0, 1):
            self.share(self.me.qd, half, self.took(self.me.qd, half))

    def last(self):
        me = self.me
        for q in (me.q, me.qx, me.qy, me.qd):
            for half in (0, 1):
                self.mail.arrived(self.slot(q, 1 - me.c, half), self.recv_pair.at[q, half], me.partner)


def enter_kernel(planes, x_ref, w_ref, j_ref, xall, wall, jall, send, rx, rp, rw, rz, rj):
    me = Spot(planes)
    mail = Mail(send)
    greet(me, [me.mate(me.qx), me.mate(me.qy), me.mate(me.qd), me.partner], True)
    others = (me.qx, me.qy, me.qd)

    def to_line(src, origin, piece):
        index = origin * 4 + piece
        mail.send(src, wall.at[index], rz.at[origin, piece], me.up, me.has_up)
        mail.send(src, wall.at[index], rz.at[origin, piece], me.down, me.has_down)

    for q in others:
        mail.send(w_ref.at[q], wall.at[me.s], rw.at[me.q], me.mate(q))
    to_line(w_ref.at[me.q], me.z, me.q)
    half_rows = x_ref.shape[0] // 2
    xg = PlaneGather(
        me, mail,
        lambda h: x_ref.at[pl.ds(h * half_rows, half_rows)],
        lambda q, c, h: xall.at[q * 2 + c, pl.ds(h * half_rows, half_rows)],
        rx, rp,
    )
    xg.start()
    for q in others:
        mail.send(j_ref.at[q], jall.at[me.q], rj.at[me.q], me.mate(q))
    mail.local(x_ref, xall.at[me.q * 2 + me.c])
    mail.local(w_ref.at[me.q], wall.at[me.s])
    mail.local(j_ref.at[me.q], jall.at[me.q])
    for q in others:
        here = wall.at[me.z * 4 + q]
        mail.arrived(here, rw.at[q], me.partner)
        to_line(here, me.z, q)

    def line_step(k):
        for piece in (me.q,) + others:
            for origin, there, on, more in (
                (me.z - k, me.z >= k, me.up, me.has_up),
                (me.z + k, me.z + k < planes, me.down, me.has_down),
            ):
                here = wall.at[origin * 4 + piece]
                sem = rz.at[origin, piece]
                pl.when(there)(functools.partial(mail.arrived, here, sem, me.partner))
                if k < planes - 1:
                    mail.send(here, here, sem, on, jnp.logical_and(there, more))

    line_step(1)
    xg.first()
    for k in range(2, planes - 1):
        line_step(k)
    xg.second()
    for q in others:
        mail.arrived(jall.at[q], rj.at[q], me.partner)
    xg.third()
    line_step(planes - 1)
    xg.last()
    mail.finish()


def enter(planes, normed, pieces, jumps):
    rows, width = normed.shape
    dma = pltpu.SemaphoreType.DMA
    return pl.pallas_call(
        functools.partial(enter_kernel, planes),
        out_shape=(
            jax.ShapeDtypeStruct((8, rows, width), normed.dtype),
            jax.ShapeDtypeStruct((planes * 4,) + pieces.shape[1:], pieces.dtype),
            jax.ShapeDtypeStruct(jumps.shape, jumps.dtype),
        ),
        in_specs=[VMEM] * 3,
        out_specs=(ANY,) * 3,
        scratch_shapes=[dma((40 + 8 * planes,)), dma((4, 2)), dma((4, 2)), dma((4,)), dma((planes, 4)), dma((4,))],
        compiler_params=pltpu.CompilerParams(collective_id=0, has_side_effects=True),
    )(normed, pieces, jumps)


def small_kernel(planes, st_ref, cr_ref, st_all, cr_all, send, rs, rc):
    me = Spot(planes)
    mail = Mail(send)
    mine = me.q * 2 + me.c
    mates = [me.at(me.z * 4 + (me.q + dq) % 4, c) for dq in range(4) for c in (me.c, 1 - me.c)][1:]
    lined = [me.at((me.s + 4 * k) % (4 * planes), me.c) for k in range(1, planes)]
    greet(me, mates + lined, False)
    for device in lined:
        mail.send(cr_ref, cr_all.at[me.z], rc.at[me.z], device)
    for device in mates:
        mail.send(st_ref, st_all.at[mine], rs.at[mine], device)
    mail.local(st_ref, st_all.at[mine])
    mail.local(cr_ref, cr_all.at[me.z])
    for k in range(1, planes):
        z = (me.z + k) % planes
        mail.arrived(cr_all.at[z], rc.at[z], me.partner)
    for k in range(1, 8):
        d = (mine + k) % 8
        mail.arrived(st_all.at[d], rs.at[d], me.partner)
    mail.finish()


def small(planes, stats, carry):
    dma = pltpu.SemaphoreType.DMA
    return pl.pallas_call(
        functools.partial(small_kernel, planes),
        out_shape=(
            jax.ShapeDtypeStruct((8,) + stats.shape, stats.dtype),
            jax.ShapeDtypeStruct((planes,) + carry.shape, carry.dtype),
        ),
        in_specs=[ANY] * 2,
        out_specs=(ANY,) * 2,
        scratch_shapes=[dma((12 + planes,)), dma((8,)), dma((planes,))],
        compiler_params=pltpu.CompilerParams(collective_id=1, has_side_effects=True),
    )(stats, carry)


def middle_kernel(planes, y_ref, w_ref, yall, wz, wp, send, ry, rp, rz, rw):
    me = Spot(planes)
    mail = Mail(send)
    greet(me, [me.mate(me.qx), me.mate(me.qy), me.mate(me.qd), me.partner], True)
    half_rows, width = y_ref.shape[0] // 2, y_ref.shape[1]
    part = planes // 2

    def hand_over(src, origin, when):
        theirs = origin // part != me.c
        if when is not None:
            theirs = jnp.logical_and(theirs, when)
        place = origin - (1 - me.c) * part
        mail.send(src, wp.at[place], rw.at[place], me.partner, theirs)

    yg = PlaneGather(
        me, mail,
        lambda h: y_ref.at[pl.ds(h * half_rows, half_rows)],
        lambda q, c, h: yall.at[
            pl.ds(h * half_rows, half_rows), pl.ds(pl.multiple_of((q * 2 + c) * width, 128), width)
        ],
        ry, rp,
    )
    mail.send(w_ref, wz.at[me.z], rz.at[me.z], me.up, me.has_up)
    mail.send(w_ref, wz.at[me.z], rz.at[me.z], me.down, me.has_down)
    yg.start()
    hand_over(w_ref, me.z, None)
    mail.local(w_ref, wz.at[me.z])
    mail.local(y_ref, yall.at[:, pl.ds(pl.multiple_of((me.q * 2 + me.c) * width, 128), width)])

    def line_step(k):
        for origin, there, on, more in (
            (me.z - k, me.z >= k, me.up, me.has_up),
            (me.z + k, me.z + k < planes, me.down, me.has_down),
        ):
            pl.when(there)(functools.partial(mail.arrived, wz.at[origin], rz.at[origin], me.partner))
            if k < planes - 1:
                mail.send(wz.at[origin], wz.at[origin], rz.at[origin], on, jnp.logical_and(there, more))
            hand_over(wz.at[origin], origin, there)

    yg.first()
    line_step(1)
    yg.second()
    for k in range(2, planes):
        if k == planes - 1:
            yg.third()
        line_step(k)
    yg.last()
    for k in range(part):
        mail.arrived(wp.at[k], rw.at[k], me.partner)
    mail.finish()


def middle(planes, mine, weights):
    rows, width = mine.shape
    dma = pltpu.SemaphoreType.DMA
    return pl.pallas_call(
        functools.partial(middle_kernel, planes),
        out_shape=(
            jax.ShapeDtypeStruct((rows, 8 * width), mine.dtype),
            jax.ShapeDtypeStruct((planes,) + weights.shape, weights.dtype),
            jax.ShapeDtypeStruct((planes // 2,) + weights.shape, weights.dtype),
        ),
        in_specs=[VMEM] * 2,
        out_specs=(ANY,) * 3,
        scratch_shapes=[dma((24 + 5 * planes,)), dma((4, 2)), dma((4, 2)), dma((planes,)), dma((planes // 2,))],
        compiler_params=pltpu.CompilerParams(collective_id=2, has_side_effects=True),
    )(mine, weights)


def leave_kernel(planes, c_ref, out, send, recv):
    me = Spot(planes)
    mail = Mail(send)
    mine = me.q * 2 + me.c
    mates = [((me.q + dq) % 4, c) for dq in (3, 1, 2, 0) for c in (me.c, 1 - me.c)]
    mates = [(q, c) for i, (q, c) in enumerate(mates) if i != 6]
    devices = [me.at(me.z * 4 + q, c) for q, c in mates]
    greet(me, devices, False)
    for (q, c), device in zip(mates, devices):
        mail.send(c_ref.at[q * 2 + c], out.at[mine], recv.at[mine], device)
    mail.local(c_ref.at[mine], out.at[mine])
    for q, c in mates:
        mail.arrived(out.at[q * 2 + c], recv.at[q * 2 + c], me.partner)
    mail.finish()


def leave(planes, blocks):
    dma = pltpu.SemaphoreType.DMA
    return pl.pallas_call(
        functools.partial(leave_kernel, planes),
        out_shape=jax.ShapeDtypeStruct(blocks.shape, blocks.dtype),
        in_specs=[VMEM],
        out_specs=ANY,
        scratch_shapes=[dma((8,)), dma((8,))],
        compiler_params=pltpu.CompilerParams(collective_id=3, has_side_effects=True),
    )(blocks)


def scan_kernel(d_ref, u_ref, p_ref, s_ref):
    def one(i, held):
        product, state = held
        decay = d_ref[i]
        product, state = product * decay, state * decay + u_ref[i]
        p_ref[i] = product
        s_ref[i] = state
        return product, state

    shape = d_ref.shape[1:]
    lax.fori_loop(
        0, d_ref.shape[0], one, (jnp.ones(shape, jnp.float32), jnp.zeros(shape, jnp.float32)), unroll=8
    )


def plane_shards(
    planes,
    tokens,
    norm_gain,
    conv_val_w,
    conv_gate_w,
    rec_gate_w,
    rec_in_w,
    conv_taps,
    conv_bias,
    conv_gain,
    short_taps,
    decay_map,
    input_map,
    decay_base,
    decay_jump,
    out_conv_w,
    out_rec_w,
):
    s, c = lax.axis_index("sp"), lax.axis_index("tp")
    z, q = s // 4, s % 4
    f32, bf16 = jnp.float32, jnp.bfloat16

    def by_mate(a):
        return a.reshape(a.shape[0], 4, a.shape[1] // 4).transpose(1, 0, 2)

    def mine(a, axis):
        size = a.shape[axis] // 4
        return lax.dynamic_slice_in_dim(a, q * size, size, axis)

    normed = norm_rows(tokens, norm_gain)
    pieces = jnp.concatenate([by_mate(w) for w in (conv_val_w, conv_gate_w, rec_gate_w, rec_in_w)], axis=2)
    xall, wall, jall = enter(planes, normed, pieces, by_mate(decay_jump))
    length = xall.shape[0] * xall.shape[1]
    cw, rw = conv_val_w.shape[1] // 4, rec_in_w.shape[1] // 4
    xall = xall.reshape(length, xall.shape[2])
    wall = wall.reshape(-1, wall.shape[2])
    jump = jall.reshape(length, rw)
    projected = jnp.dot(xall, wall, preferred_element_type=f32).astype(bf16)
    glu = glu_of(projected[:, :cw], projected[:, cw : 2 * cw])
    rec_gate, rec_in = projected[:, 2 * cw : 2 * cw + rw], projected[:, 2 * cw + rw :]
    conv_lags, short_lags = conv_taps.shape[0] - 1, short_taps.shape[0] - 1
    edge = passed_along(jnp.concatenate([glu[-conv_lags:], rec_in[-conv_lags:]], axis=1), "sp", 4)

    filtered = causal_window(edge[:, :cw], glu, mine(conv_taps, 1)) + mine(conv_bias, 0)[None, :]
    local_sum = jnp.sum(filtered, axis=1)
    off = filtered - (local_sum / cw)[:, None]
    local_spread = jnp.sum(off * off, axis=1)
    stats = jnp.stack([local_sum, local_spread]).reshape(-1, 128)

    smoothed = causal_window(edge[-short_lags:, cw:], rec_in, mine(short_taps, 1)).astype(bf16)
    heads, size = decay_map.shape[0] // 4, decay_map.shape[1]
    eye = jnp.eye(heads, dtype=bf16)

    def widened(m):
        return (mine(m, 0)[:, :, None, :] * eye[:, None, :, None]).reshape(rw, rw)

    gates = jax.nn.sigmoid(
        jnp.dot(
            smoothed,
            jnp.concatenate([widened(decay_map), widened(input_map)], axis=1),
            preferred_element_type=f32,
        )
    )
    retain, admit = gates[:, :rw], gates[:, rw:]
    log_decay = -RATE_SCALE * retain * jax.nn.softplus(-mine(decay_base, 0))[None, :] + jump
    decay = jnp.exp(log_decay)
    inflow = jnp.sqrt(-jnp.expm1(2.0 * log_decay)) * admit * smoothed.astype(f32)
    steps = length // SEGMENTS

    def by_step(a):
        return a.reshape(SEGMENTS, steps, rw).transpose(1, 0, 2)

    products, states = pl.pallas_call(
        scan_kernel,
        out_shape=(jax.ShapeDtypeStruct((steps, SEGMENTS, rw), f32),) * 2,
        in_specs=[VMEM] * 2,
        out_specs=(VMEM,) * 2,
    )(by_step(decay), by_step(inflow))
    seg_p, seg_s = products[-1], states[-1]
    total = (jnp.ones((rw,), f32), jnp.zeros((rw,), f32))
    for i in range(SEGMENTS):
        total = chain_step(total, (seg_p[i], seg_s[i]))
    st_all, cr_all = small(planes, stats, jnp.stack(total))

    st_all = st_all.reshape(8, 2, length)
    width = 8 * cw
    mean = jnp.sum(st_all[:, 0], axis=0) / width
    shift = st_all[:, 0] / cw - mean[None]
    spread = jnp.sum(st_all[:, 1] + cw * shift * shift, axis=0) / width
    conv_out = jax.nn.silu(
        (filtered - mean[:, None]) * lax.rsqrt(spread + 1e-05)[:, None] * mine(conv_gain, 0)[None, :]
    ).astype(bf16)

    held = jnp.zeros((rw,), f32)
    for i in range(planes - 1):
        held = jnp.where(i < z, cr_all[i, 0] * held + cr_all[i, 1], held)
    entering = []
    for i in range(SEGMENTS):
        entering.append(held)
        held = seg_p[i] * held + seg_s[i]
    state = (states + products * jnp.stack(entering)[None]).transpose(1, 0, 2).reshape(length, rw)
    rec_out = (jax.nn.gelu(rec_gate.astype(f32)) * state).astype(bf16)
    fill = -(cw + rw) % 128
    block = jnp.concatenate([conv_out, rec_out, jnp.zeros((length, fill), bf16)], axis=1)

    cols = out_conv_w.shape[1]
    rows_by_mate = jnp.concatenate(
        [out_conv_w.reshape(4, cw, cols), out_rec_w.reshape(4, rw, cols)], axis=1
    ).reshape(-1, cols)
    yall, wz, wp = middle(planes, block, rows_by_mate)
    part = planes // 2
    own = lax.dynamic_slice_in_dim(wz, c * part, part, 0)
    both = jnp.stack([jnp.where(c == 0, own, wp), jnp.where(c == 0, wp, own)])
    both = both.reshape(2, part, 4, cw + rw, cols).transpose(2, 0, 3, 1, 4)
    both = jnp.pad(both, ((0, 0), (0, 0), (0, fill), (0, 0), (0, 0))).reshape(-1, part * cols)
    mixed = jnp.dot(yall, both, preferred_element_type=f32).astype(bf16)
    out = leave(planes, mixed.reshape(8, length // 8, part * cols))
    out = out.reshape(4, 2, length // 8, part, cols).transpose(2, 1, 3, 0, 4)
    return out.reshape(length // 8, -1)


def solution(mesh):
    in_specs = (
        P(("sp", "tp"), None),
        P(),
        P("sp", "tp"),
        P("sp", "tp"),
        P("sp", "tp"),
        P("sp", "tp"),
        P(None, "tp"),
        P("tp"),
        P("tp"),
        P(None, "tp"),
        P("tp", None, None),
        P("tp", None, None),
        P("tp"),
        P("sp", "tp"),
        P("tp", "sp"),
        P("tp", "sp"),
    )
    out_specs = P(("sp", "tp"), None)
    count = mesh.shape["sp"]
    planar = mesh.shape["tp"] == 2 and count % 8 == 0
    body = functools.partial(plane_shards, count // 4) if planar else shards
    return jax.shard_map(body, mesh=mesh, in_specs=in_specs, out_specs=out_specs, check_vma=False)
```

```python
import functools

import jax
import jax.numpy as jnp
from jax import lax
from jax.experimental import pallas as pl
from jax.experimental.pallas import tpu as pltpu
from jax.sharding import PartitionSpec as P

CONV_WIDTH = 1024


RATE_SCALE = 8.0


def passed_along(value, axis, by):
    count = lax.axis_size(axis)
    pairs = [(i, i + by) for i in range(count) if 0 <= i + by < count]
    return lax.ppermute(value, axis, pairs)


def prefix(part, axis, combine, identity):
    place = lax.axis_index(axis)
    gathered = jax.tree.map(lambda a: lax.all_gather(a, axis), part)
    state = jax.tree.map(lambda a, e: jnp.zeros_like(a) + jnp.asarray(e, a.dtype), part, identity)

    def one(step, state):
        return combine(
            state, jax.tree.map(lambda a: lax.dynamic_index_in_dim(a, step, 0, False), gathered)
        )

    return lax.fori_loop(0, place, one, state)


def norm_rows(values, gain):
    widened = values.astype(jnp.float32)
    inverse = lax.rsqrt(jnp.mean(widened * widened, axis=-1, keepdims=True) + 1e-06)
    return (widened * inverse * gain).astype(jnp.bfloat16)


def causal_window(edge, current, weights):
    extended = jnp.concatenate([edge, current], axis=0).astype(jnp.float32)
    taps_wide = weights.astype(jnp.float32)
    length = current.shape[0]
    result = jnp.zeros((length, current.shape[1]), jnp.float32)
    for lag_index in range(weights.shape[0]):
        result = result + taps_wide[lag_index][None, :] * extended[lag_index : lag_index + length]
    return result


def chain_step(earlier, latter):
    return (earlier[0] * latter[0], latter[0] * earlier[1] + latter[1])


def glu_of(conv_val, conv_gate):
    return (conv_val.astype(jnp.float32) * jax.nn.sigmoid(conv_gate.astype(jnp.float32))).astype(
        jnp.bfloat16
    )


def shards(
    tokens,
    norm_gain,
    conv_val_w,
    conv_gate_w,
    rec_gate_w,
    rec_in_w,
    conv_taps,
    conv_bias,
    conv_gain,
    short_taps,
    decay_map,
    input_map,
    decay_base,
    decay_jump,
    out_conv_w,
    out_rec_w,
):
    rec_cols = rec_in_w.shape[1]
    conv_lags = conv_taps.shape[0] - 1
    short_lags = short_taps.shape[0] - 1
    normed = norm_rows(tokens, norm_gain)
    val_full, gate_full = (
        lax.all_gather(conv_val_w, "sp", axis=0, tiled=True),
        lax.all_gather(conv_gate_w, "sp", axis=0, tiled=True),
    )
    all_rows = lax.all_gather(normed, "tp", axis=0, tiled=True)
    conv_val = jnp.dot(all_rows, val_full, preferred_element_type=jnp.float32).astype(jnp.bfloat16)
    conv_gate = jnp.dot(all_rows, gate_full, preferred_element_type=jnp.float32).astype(
        jnp.bfloat16
    )
    glu = glu_of(conv_val, conv_gate)
    conv_edge = passed_along(glu[-conv_lags:], "sp", 1)
    rgate_full, rin_full = (
        lax.all_gather(rec_gate_w, "sp", axis=0, tiled=True),
        lax.all_gather(rec_in_w, "sp", axis=0, tiled=True),
    )
    rec_gate = jnp.dot(all_rows, rgate_full, preferred_element_type=jnp.float32).astype(
        jnp.bfloat16
    )
    rec_in = jnp.dot(all_rows, rin_full, preferred_element_type=jnp.float32).astype(jnp.bfloat16)
    rec_edge = passed_along(rec_in[-short_lags:], "sp", 1)
    filtered = causal_window(conv_edge, glu, conv_taps) + conv_bias[None, :]
    row_total = lax.psum(jnp.sum(filtered, axis=1), "tp")
    centered = filtered - (row_total / CONV_WIDTH)[:, None]
    spread = lax.psum(jnp.sum(centered * centered, axis=1), "tp") / CONV_WIDTH
    conv_out = jax.nn.silu(centered * lax.rsqrt(spread + 1e-05)[:, None] * conv_gain).astype(
        jnp.bfloat16
    )
    smoothed = causal_window(rec_edge, rec_in, short_taps).astype(jnp.bfloat16)
    length = smoothed.shape[0]
    grouped = smoothed.reshape(length, decay_map.shape[0], decay_map.shape[1])
    retain = jax.nn.sigmoid(
        jnp.einsum("thi,hio->tho", grouped, decay_map, preferred_element_type=jnp.float32).reshape(
            length, rec_cols
        )
    )
    admit = jax.nn.sigmoid(
        jnp.einsum("thi,hio->tho", grouped, input_map, preferred_element_type=jnp.float32).reshape(
            length, rec_cols
        )
    )
    log_decay = -RATE_SCALE * retain * jax.nn.softplus(-decay_base)[None, :] + decay_jump
    decay = jnp.exp(log_decay)
    inflow = jnp.sqrt(-jnp.expm1(2.0 * log_decay)) * admit * smoothed.astype(jnp.float32)
    products, local_state = lax.associative_scan(chain_step, (decay, inflow), axis=0)
    entering = prefix(
        (products[-1], local_state[-1]),
        "sp",
        chain_step,
        (jnp.ones((rec_cols,), jnp.float32), jnp.zeros((rec_cols,), jnp.float32)),
    )
    state = local_state + products * entering[1][None, :]
    rec_out = (jax.nn.gelu(rec_gate.astype(jnp.float32)) * state).astype(jnp.bfloat16)
    conv_full, rec_full = (
        lax.all_gather(out_conv_w, "sp", axis=1, tiled=True),
        lax.all_gather(out_rec_w, "sp", axis=1, tiled=True),
    )
    return lax.psum_scatter(
        (
            jnp.dot(conv_out, conv_full, preferred_element_type=jnp.float32)
            + jnp.dot(rec_out, rec_full, preferred_element_type=jnp.float32)
        ).astype(jnp.bfloat16),
        "tp",
        scatter_dimension=0,
        tiled=True,
    )


MESH = pl.DeviceIdType.MESH
ANY = pl.BlockSpec(memory_space=pl.ANY)
VMEM = pl.BlockSpec(memory_space=pltpu.VMEM)
SEGMENTS = 8


class Spot:
    def __init__(self, planes):
        self.s, self.c = lax.axis_index("sp"), lax.axis_index("tp")
        self.z, self.q = self.s // 4, self.s % 4
        self.qx = self.q + 1 - 2 * (self.q % 2)
        self.qy = (self.q + 2) % 4
        self.qd = 3 - self.q
        self.has_up, self.has_down = self.z < planes - 1, self.z > 0
        self.up, self.down = self.at(self.s + 4, self.c), self.at(self.s - 4, self.c)
        self.partner = self.at(self.s, 1 - self.c)

    def at(self, s, c):
        return {"sp": s, "tp": c}

    def mate(self, q):
        return self.at(self.z * 4 + q, self.c)


class Mail:
    def __init__(self, send_sem):
        self.send_sem, self.count, self.open = send_sem, 0, []

    def send(self, src, dst, recv, device, when=None):
        copy = pltpu.make_async_remote_copy(
            src_ref=src, dst_ref=dst, send_sem=self.send_sem.at[self.count],
            recv_sem=recv, device_id=device, device_id_type=MESH,
        )
        self.count += 1
        self.open.append((copy.wait_send, when))
        if when is None:
            copy.start()
        else:
            pl.when(when)(copy.start)

    def local(self, src, dst):
        copy = pltpu.make_async_copy(src, dst, self.send_sem.at[self.count])
        self.count += 1
        copy.start()
        self.open.append((copy.wait, None))

    def arrived(self, dst, recv, device):
        pltpu.make_async_remote_copy(
            src_ref=dst, dst_ref=dst, send_sem=self.send_sem.at[0],
            recv_sem=recv, device_id=device, device_id_type=MESH,
        ).wait_recv()

    def finish(self):
        for wait, when in self.open:
            if when is None:
                wait()
            else:
                pl.when(when)(wait)


def greet(me, devices, line):
    barrier = pltpu.get_barrier_semaphore()
    for device in devices:
        pl.semaphore_signal(barrier, inc=1, device_id=device, device_id_type=MESH)
    amount = len(devices)
    if line:
        for has, device in ((me.has_up, me.up), (me.has_down, me.down)):
            @pl.when(has)
            def _():
                pl.semaphore_signal(barrier, inc=1, device_id=device, device_id_type=MESH)
        amount = amount + me.has_up.astype(jnp.int32) + me.has_down.astype(jnp.int32)
    pl.semaphore_wait(barrier, amount)


class PlaneGather:
    def __init__(self, me, mail, own, slot, recv, recv_pair):
        self.me, self.mail, self.own, self.slot = me, mail, own, slot
        self.recv, self.recv_pair = recv, recv_pair

    def start(self):
        me, mail = self.me, self.mail
        for h in (0, 1):
            for q, half in ((me.qx, h), (me.qy, 1 - h)):
                mail.send(self.own(half), self.slot(me.q, me.c, half), self.recv.at[me.q, half], me.mate(q))
        for half in (0, 1):
            mail.send(self.own(half), self.slot(me.q, me.c, half), self.recv_pair.at[me.q, half], me.partner)

    def took(self, q, half):
        me, mail = self.me, self.mail
        here = self.slot(q, me.c, half)
        mail.arrived(here, self.recv.at[q, half], me.partner)
        return here

    def share(self, q, half, here):
        self.mail.send(here, here, self.recv_pair.at[q, half], self.me.partner)

    def first(self):
        me = self.me
        for q, half, to in ((me.qx, 0, me.qy), (me.qy, 1, me.qx)):
            here = self.took(q, half)
            self.mail.send(here, here, self.recv.at[q, half], me.mate(to))
            self.share(q, half, here)

    def second(self):
        for q, half in ((self.me.qx, 1), (self.me.qy, 0)):
            self.share(q, half, self.took(q, half))

    def third(self):
        for half in (0, 1):
            self.share(self.me.qd, half, self.took(self.me.qd, half))

    def last(self):
        me = self.me
        for q in (me.q, me.qx, me.qy, me.qd):
            for half in (0, 1):
                self.mail.arrived(self.slot(q, 1 - me.c, half), self.recv_pair.at[q, half], me.partner)


def enter_kernel(planes, x_ref, w_ref, j_ref, xall, wall, jall, send, rx, rp, rw, rz, rj):
    me = Spot(planes)
    mail = Mail(send)
    greet(me, [me.mate(me.qx), me.mate(me.qy), me.mate(me.qd), me.partner], True)
    others = (me.qx, me.qy, me.qd)

    def to_line(src, origin, piece):
        index = origin * 4 + piece
        mail.send(src, wall.at[index], rz.at[origin, piece], me.up, me.has_up)
        mail.send(src, wall.at[index], rz.at[origin, piece], me.down, me.has_down)

    for q in others:
        mail.send(w_ref.at[q], wall.at[me.s], rw.at[me.q], me.mate(q))
    to_line(w_ref.at[me.q], me.z, me.q)
    half_rows = x_ref.shape[0] // 2
    xg = PlaneGather(
        me, mail,
        lambda h: x_ref.at[pl.ds(h * half_rows, half_rows)],
        lambda q, c, h: xall.at[q * 2 + c, pl.ds(h * half_rows, half_rows)],
        rx, rp,
    )
    xg.start()
    for q in others:
        mail.send(j_ref.at[q], jall.at[me.q], rj.at[me.q], me.mate(q))
    mail.local(x_ref, xall.at[me.q * 2 + me.c])
    mail.local(w_ref.at[me.q], wall.at[me.s])
    mail.local(j_ref.at[me.q], jall.at[me.q])
    for q in others:
        here = wall.at[me.z * 4 + q]
        mail.arrived(here, rw.at[q], me.partner)
        to_line(here, me.z, q)

    def line_step(k):
        for piece in (me.q,) + others:
            for origin, there, on, more in (
                (me.z - k, me.z >= k, me.up, me.has_up),
                (me.z + k, me.z + k < planes, me.down, me.has_down),
            ):
                here = wall.at[origin * 4 + piece]
                sem = rz.at[origin, piece]
                pl.when(there)(functools.partial(mail.arrived, here, sem, me.partner))
                if k < planes - 1:
                    mail.send(here, here, sem, on, jnp.logical_and(there, more))

    line_step(1)
    xg.first()
    for k in range(2, planes - 1):
        line_step(k)
    xg.second()
    for q in others:
        mail.arrived(jall.at[q], rj.at[q], me.partner)
    xg.third()
    line_step(planes - 1)
    xg.last()
    mail.finish()


def enter(planes, normed, pieces, jumps):
    rows, width = normed.shape
    dma = pltpu.SemaphoreType.DMA
    return pl.pallas_call(
        functools.partial(enter_kernel, planes),
        out_shape=(
            jax.ShapeDtypeStruct((8, rows, width), normed.dtype),
            jax.ShapeDtypeStruct((planes * 4,) + pieces.shape[1:], pieces.dtype),
            jax.ShapeDtypeStruct(jumps.shape, jumps.dtype),
        ),
        in_specs=[VMEM] * 3,
        out_specs=(ANY,) * 3,
        scratch_shapes=[dma((40 + 8 * planes,)), dma((4, 2)), dma((4, 2)), dma((4,)), dma((planes, 4)), dma((4,))],
        compiler_params=pltpu.CompilerParams(collective_id=0, has_side_effects=True),
    )(normed, pieces, jumps)


def minus_expm1(y):
    series = 1.0 + y * (1.0 / 8.0)
    for n in (7.0, 6.0, 5.0, 4.0, 3.0, 2.0):
        series = 1.0 + y * (1.0 / n) * series
    return jnp.where(y > -0.35, -y * series, 1.0 - jnp.exp(y))


def gelu(v):
    return 0.5 * v * (1.0 + jnp.tanh(0.7978845608028654 * (v + 0.044715 * v * v * v)))


def core_kernel(
    planes, lags, proj, jump, cpar, rpar, dmap, imap, w_ref,
    out, wz, wp, yall, halo, gext, rext, filt, dec, inf, maps, stat, st_all, carry, cr_all,
    send, ry, rp, rz, rw, rh, rs, rc,
):
    me = Spot(planes)
    mail = Mail(send)
    c_lags, s_lags = lags
    f32, bf16 = jnp.float32, jnp.bfloat16
    length = proj.shape[0]
    cw = gext.shape[1]
    rwid = jump.shape[1]
    seg = length // SEGMENTS
    top = halo.shape[0]
    fold = dec.shape[0]
    part = planes // 2
    width = yall.shape[1] // 8
    mine = me.q * 2 + me.c
    mates = [me.at(me.z * 4 + (me.q + dq) % 4, c) for dq in range(4) for c in (me.c, 1 - me.c)][1:]
    lined = [me.at((me.s + 4 * k) % (4 * planes), me.c) for k in range(1, planes)]
    greet(me, mates + lined, False)

    def hand_over(src, origin, when):
        theirs = origin // part != me.c
        if when is not None:
            theirs = jnp.logical_and(theirs, when)
        place = origin - (1 - me.c) * part
        mail.send(src, wp.at[place], rw.at[place], me.partner, theirs)

    mail.send(proj.at[pl.ds(length - top, top)], halo, rh.at[0], me.up, me.has_up)
    mail.send(w_ref, wz.at[me.z], rz.at[me.z], me.up, me.has_up)
    mail.send(w_ref, wz.at[me.z], rz.at[me.z], me.down, me.has_down)
    hand_over(w_ref, me.z, None)
    mail.local(w_ref, wz.at[me.z])

    maps[...] = jnp.zeros_like(maps)
    size = dmap.shape[1]
    heads = rwid // size
    for h in range(heads):
        spot = pl.ds(h * size, size)
        maps[spot, pl.ds(h * size, size)] = dmap[me.q * heads + h]
        maps[spot, pl.ds(fold * 128 + h * size, size)] = imap[me.q * heads + h]

    def columns(ref, row, count):
        val = ref[pl.ds(row, count), pl.ds(0, cw)].astype(f32)
        gate = ref[pl.ds(row, count), pl.ds(cw, cw)].astype(f32)
        return (val * jax.nn.sigmoid(gate)).astype(bf16).astype(f32)

    rec_at, gate_at = 2 * cw + rwid, 2 * cw

    @pl.loop(0, SEGMENTS)
    def _(i):
        base = pl.multiple_of(i * seg, 16)
        gext[pl.ds(pl.multiple_of(base + top, 8), seg)] = columns(proj, base, seg)
        rext[pl.ds(pl.multiple_of(base + top, 8), seg)] = proj[pl.ds(base, seg), pl.ds(rec_at, rwid)].astype(f32)

    @pl.when(me.has_down)
    def _():
        mail.arrived(halo, rh.at[0], me.partner)
        gext[pl.ds(0, top)] = columns(halo, 0, top)
        rext[pl.ds(0, top)] = halo[:, pl.ds(rec_at, rwid)].astype(f32)

    @pl.when(jnp.logical_not(me.has_down))
    def _():
        gext[pl.ds(0, top)] = jnp.zeros((top, cw), f32)
        rext[pl.ds(0, top)] = jnp.zeros((top, rwid), f32)

    softened = rpar[me.q, pl.ds(s_lags + 1, 1), :]

    @pl.loop(0, SEGMENTS)
    def _(i):
        base = pl.multiple_of(i * seg, 8)
        window = rext[pl.ds(pl.multiple_of(base + top - 8, 8), seg + 8)]
        smooth = jnp.zeros((seg, rwid), f32)
        for k in range(s_lags + 1):
            smooth = smooth + rpar[me.q, pl.ds(k, 1), :] * window[8 - s_lags + k : 8 - s_lags + k + seg]
        smooth = smooth.astype(bf16)
        gates = jax.nn.sigmoid(jnp.dot(smooth, maps[...], preferred_element_type=f32))
        retain, admit = gates[:, :rwid], gates[:, fold * 128 : fold * 128 + rwid]
        log_decay = jump[pl.ds(base, seg)] - retain * softened
        decay = jnp.exp(log_decay)
        inflow = jnp.sqrt(minus_expm1(2.0 * log_decay)) * admit * smooth.astype(f32)
        for f in range(fold):
            w = min(128, rwid - f * 128)
            dec[f, pl.ds(base, seg), pl.ds(0, w)] = decay[:, f * 128 : f * 128 + w]
            inf[f, pl.ds(base, seg), pl.ds(0, w)] = inflow[:, f * 128 : f * 128 + w]

    def one(i, held):
        after = []
        for f in range(fold):
            at = pl.ds(i, SEGMENTS, stride=seg)
            d = dec.at[f][at, :]
            product, state = held[2 * f] * d, held[2 * f + 1] * d + inf.at[f][at, :]
            dec.at[f][at, :] = product
            inf.at[f][at, :] = state
            after += [product, state]
        return tuple(after)

    flat = (SEGMENTS, 128)
    ends = lax.fori_loop(0, seg, one, (jnp.ones(flat, f32), jnp.zeros(flat, f32)) * fold, unroll=8)
    for f in range(fold):
        product, state = jnp.ones((1, 128), f32), jnp.zeros((1, 128), f32)
        for i in range(SEGMENTS):
            p, s = ends[2 * f][i : i + 1], ends[2 * f + 1][i : i + 1]
            product, state = product * p, p * state + s
        carry[pl.ds(2 * f, 1)] = product
        carry[pl.ds(2 * f + 1, 1)] = state
    for device in lined:
        mail.send(carry, cr_all.at[me.z], rc.at[me.z], device)

    @pl.loop(0, length // 64)
    def _(i):
        base = pl.multiple_of(i * 64, 8)
        window = gext[pl.ds(base, 64 + top)]
        total = jnp.zeros((64, cw), f32) + cpar[pl.ds(c_lags + 1, 1), :]
        for k in range(c_lags + 1):
            begin = top - c_lags + k
            total = total + cpar[pl.ds(k, 1), :] * window[begin : begin + 64]
        filt[pl.ds(base, 64)] = total
        part_sum = jnp.sum(total, axis=1, keepdims=True)
        off = total - part_sum * (1.0 / cw)
        lane = lax.broadcasted_iota(jnp.int32, (64, 128), 1)
        spread = jnp.sum(off * off, axis=1, keepdims=True)
        stat[pl.ds(base, 64)] = jnp.where(lane == 0, part_sum, spread)

    packed = stat[...].T
    st_all[mine] = packed[0:8]
    for device in mates:
        mail.send(st_all.at[mine], st_all.at[mine], rs.at[mine], device)

    def line_step(k):
        for origin, there, on, more in (
            (me.z - k, me.z >= k, me.up, me.has_up),
            (me.z + k, me.z + k < planes, me.down, me.has_down),
        ):
            pl.when(there)(functools.partial(mail.arrived, wz.at[origin], rz.at[origin], me.partner))
            if k < planes - 1:
                mail.send(wz.at[origin], wz.at[origin], rz.at[origin], on, jnp.logical_and(there, more))
            hand_over(wz.at[origin], origin, there)

    for k in range(1, planes):
        z = (me.z + k) % planes
        mail.arrived(cr_all.at[z], rc.at[z], me.partner)
    cr_all[me.z] = carry[...]
    entering = []
    for f in range(fold):
        held = jnp.zeros((1, 128), f32)
        for j in range(planes - 1):
            after = cr_all[j, pl.ds(2 * f, 1)] * held + cr_all[j, pl.ds(2 * f + 1, 1)]
            held = jnp.where(j < me.z, after, held)
        for i in range(SEGMENTS):
            entering.append(held)
            held = ends[2 * f][i : i + 1] * held + ends[2 * f + 1][i : i + 1]
    own_at = pl.multiple_of(mine * width, 128)
    for i in range(SEGMENTS):
        rows = pl.ds(i * seg, seg)
        state = [dec[f, rows] * entering[f * SEGMENTS + i] + inf[f, rows] for f in range(fold)]
        state = jnp.concatenate(state, axis=1)[:, :rwid]
        result = gelu(proj[rows, pl.ds(gate_at, rwid)].astype(f32)) * state
        fill = jnp.zeros((seg, width - cw - rwid), f32)
        yall[rows, pl.ds(pl.multiple_of(own_at + cw, 128), width - cw)] = jnp.concatenate([result, fill], axis=1).astype(bf16)

    for k in range(1, 8):
        d = (mine + k) % 8
        mail.arrived(st_all.at[d], rs.at[d], me.partner)
    total = sum(st_all[d, 0:1, :] for d in range(8))
    mean = total * (1.0 / (8 * cw))
    spread = jnp.zeros_like(mean)
    for d in range(8):
        shift = st_all[d, 0:1, :] * (1.0 / cw) - mean
        spread = spread + st_all[d, 1:2, :] + cw * shift * shift
    scale = lax.rsqrt(spread * (1.0 / (8 * cw)) + 1e-05)
    row = lax.broadcasted_iota(jnp.int32, (128, length), 0)
    stat[...] = jnp.where(row == 0, mean, scale).T

    @pl.loop(0, SEGMENTS)
    def _(i):
        rows = pl.ds(pl.multiple_of(i * seg, 16), seg)
        pair = stat[rows]
        v = (filt[rows] - pair[:, 0:1]) * pair[:, 1:2] * cpar[pl.ds(c_lags + 2, 1), :]
        yall[rows, pl.ds(own_at, cw)] = (v * jax.nn.sigmoid(v)).astype(bf16)

    half_rows = length // 2

    def slot(q, c, h):
        return yall.at[pl.ds(h * half_rows, half_rows), pl.ds(pl.multiple_of((q * 2 + c) * width, 128), width)]

    yg = PlaneGather(me, mail, lambda h: slot(me.q, me.c, h), slot, ry, rp)
    yg.start()
    line_step(1)
    yg.first()
    for k in range(2, planes):
        line_step(k)
        if k == 2:
            yg.second()
    yg.third()
    yg.last()
    for k in range(part):
        mail.arrived(wp.at[k], rw.at[k], me.partner)
    mail.finish()

    used, cols = cw + rwid, w_ref.shape[1]
    tile = length // 8

    @pl.loop(0, 8)
    def _(i):
        rows = pl.ds(pl.multiple_of(i * tile, 16), tile)
        for k in range(part):
            total = jnp.zeros((tile, cols), f32)
            for q in range(4):
                for c, block in ((me.c, wz.at[me.c * part + k]), (1 - me.c, wp.at[k])):
                    left = yall[rows, pl.ds(pl.multiple_of((q * 2 + c) * width, 128), width)]
                    total = total + jnp.dot(
                        left[:, :used], block[pl.ds(q * used, used)], preferred_element_type=f32
                    )
            out[i, :, pl.ds(k * cols, cols)] = total.astype(bf16)


def core(planes, proj, jump, cpar, rpar, dmap, imap, weights, lags, cw):
    length, rwid = jump.shape
    used, cols = cw + rwid, weights.shape[1]
    width = used + -used % 128
    fold = (rwid + 127) // 128
    f32, bf16 = jnp.float32, jnp.bfloat16
    dma, vmem = pltpu.SemaphoreType.DMA, pltpu.VMEM
    top = lags[0] + -lags[0] % 16
    part = planes // 2
    return pl.pallas_call(
        functools.partial(core_kernel, planes, lags),
        out_shape=jax.ShapeDtypeStruct((8, length // 8, part * cols), bf16),
        in_specs=[VMEM] * 7,
        out_specs=VMEM,
        scratch_shapes=[
            vmem((planes,) + weights.shape, bf16),
            vmem((part,) + weights.shape, bf16),
            vmem((length, 8 * width), bf16),
            vmem((top, proj.shape[1]), bf16),
            vmem((top + length, cw), f32),
            vmem((top + length, rwid), f32),
            vmem((length, cw), f32),
            vmem((fold, length, 128), f32),
            vmem((fold, length, 128), f32),
            vmem((rwid, 2 * fold * 128), bf16),
            vmem((length, 128), f32),
            vmem((8, 8, length), f32),
            vmem((8, 128), f32),
            vmem((planes, 8, 128), f32),
            dma((48 + 8 * planes,)), dma((4, 2)), dma((4, 2)), dma((planes,)), dma((part,)),
            dma((1,)), dma((8,)), dma((planes,)),
        ],
        compiler_params=pltpu.CompilerParams(
            collective_id=2, has_side_effects=True, vmem_limit_bytes=60 * 1024 * 1024
        ),
    )(proj, jump, cpar, rpar, dmap, imap, weights)


def leave_kernel(planes, c_ref, out, send, recv):
    me = Spot(planes)
    mail = Mail(send)
    mine = me.q * 2 + me.c
    mates = [((me.q + dq) % 4, c) for dq in (3, 1, 2, 0) for c in (me.c, 1 - me.c)]
    mates = [(q, c) for i, (q, c) in enumerate(mates) if i != 6]
    devices = [me.at(me.z * 4 + q, c) for q, c in mates]
    greet(me, devices, False)
    for (q, c), device in zip(mates, devices):
        mail.send(c_ref.at[q * 2 + c], out.at[mine], recv.at[mine], device)
    mail.local(c_ref.at[mine], out.at[mine])
    for q, c in mates:
        mail.arrived(out.at[q * 2 + c], recv.at[q * 2 + c], me.partner)
    mail.finish()


def leave(planes, blocks):
    dma = pltpu.SemaphoreType.DMA
    return pl.pallas_call(
        functools.partial(leave_kernel, planes),
        out_shape=jax.ShapeDtypeStruct(blocks.shape, blocks.dtype),
        in_specs=[VMEM],
        out_specs=ANY,
        scratch_shapes=[dma((8,)), dma((8,))],
        compiler_params=pltpu.CompilerParams(collective_id=3, has_side_effects=True),
    )(blocks)


def plane_shards(
    planes,
    tokens,
    norm_gain,
    conv_val_w,
    conv_gate_w,
    rec_gate_w,
    rec_in_w,
    conv_taps,
    conv_bias,
    conv_gain,
    short_taps,
    decay_map,
    input_map,
    decay_base,
    decay_jump,
    out_conv_w,
    out_rec_w,
):
    s, c = lax.axis_index("sp"), lax.axis_index("tp")
    z, q = s // 4, s % 4
    f32, bf16 = jnp.float32, jnp.bfloat16

    def by_mate(a):
        return a.reshape(a.shape[0], 4, a.shape[1] // 4).transpose(1, 0, 2)

    def mine(a, axis):
        size = a.shape[axis] // 4
        return lax.dynamic_slice_in_dim(a, q * size, size, axis)

    normed = norm_rows(tokens, norm_gain)
    pieces = jnp.concatenate([by_mate(w) for w in (conv_val_w, conv_gate_w, rec_gate_w, rec_in_w)], axis=2)
    xall, wall, jall = enter(planes, normed, pieces, by_mate(decay_jump))
    length = xall.shape[0] * xall.shape[1]
    cw, rw = conv_val_w.shape[1] // 4, rec_in_w.shape[1] // 4
    xall = xall.reshape(length, xall.shape[2])
    wall = wall.reshape(-1, wall.shape[2])
    jump = jall.reshape(length, rw)
    projected = jnp.dot(xall, wall, preferred_element_type=f32).astype(bf16)
    cols = out_conv_w.shape[1]
    rows_by_mate = jnp.concatenate(
        [out_conv_w.reshape(4, cw, cols), out_rec_w.reshape(4, rw, cols)], axis=1
    ).reshape(-1, cols)
    cpar = mine(jnp.concatenate([conv_taps.astype(f32), conv_bias[None], conv_gain[None]]), 1)
    rpar = by_mate(jnp.concatenate([short_taps.astype(f32), RATE_SCALE * jax.nn.softplus(-decay_base)[None]]))
    lags = (conv_taps.shape[0] - 1, short_taps.shape[0] - 1)
    mixed = core(planes, projected, jump, cpar, rpar, decay_map, input_map, rows_by_mate, lags, cw)
    out = leave(planes, mixed)
    part = planes // 2
    out = out.reshape(4, 2, length // 8, part, cols).transpose(2, 1, 3, 0, 4)
    return out.reshape(length // 8, -1)


def solution(mesh):
    in_specs = (
        P(("sp", "tp"), None),
        P(),
        P("sp", "tp"),
        P("sp", "tp"),
        P("sp", "tp"),
        P("sp", "tp"),
        P(None, "tp"),
        P("tp"),
        P("tp"),
        P(None, "tp"),
        P("tp", None, None),
        P("tp", None, None),
        P("tp"),
        P("sp", "tp"),
        P("tp", "sp"),
        P("tp", "sp"),
    )
    out_specs = P(("sp", "tp"), None)
    count = mesh.shape["sp"]
    planar = mesh.shape["tp"] == 2 and count % 8 == 0
    body = functools.partial(plane_shards, count // 4) if planar else shards
    return jax.shard_map(body, mesh=mesh, in_specs=in_specs, out_specs=out_specs, check_vma=False)
```

```python
import functools

import jax
import jax.numpy as jnp
from jax import lax
from jax.experimental import pallas as pl
from jax.experimental.pallas import tpu as pltpu
from jax.sharding import PartitionSpec as P

CONV_WIDTH = 1024


RATE_SCALE = 8.0


def passed_along(value, axis, by):
    count = lax.axis_size(axis)
    pairs = [(i, i + by) for i in range(count) if 0 <= i + by < count]
    return lax.ppermute(value, axis, pairs)


def prefix(part, axis, combine, identity):
    place = lax.axis_index(axis)
    gathered = jax.tree.map(lambda a: lax.all_gather(a, axis), part)
    state = jax.tree.map(lambda a, e: jnp.zeros_like(a) + jnp.asarray(e, a.dtype), part, identity)

    def one(step, state):
        return combine(
            state, jax.tree.map(lambda a: lax.dynamic_index_in_dim(a, step, 0, False), gathered)
        )

    return lax.fori_loop(0, place, one, state)


def norm_rows(values, gain):
    widened = values.astype(jnp.float32)
    inverse = lax.rsqrt(jnp.mean(widened * widened, axis=-1, keepdims=True) + 1e-06)
    return (widened * inverse * gain).astype(jnp.bfloat16)


def causal_window(edge, current, weights):
    extended = jnp.concatenate([edge, current], axis=0).astype(jnp.float32)
    taps_wide = weights.astype(jnp.float32)
    length = current.shape[0]
    result = jnp.zeros((length, current.shape[1]), jnp.float32)
    for lag_index in range(weights.shape[0]):
        result = result + taps_wide[lag_index][None, :] * extended[lag_index : lag_index + length]
    return result


def chain_step(earlier, latter):
    return (earlier[0] * latter[0], latter[0] * earlier[1] + latter[1])


def glu_of(conv_val, conv_gate):
    return (conv_val.astype(jnp.float32) * jax.nn.sigmoid(conv_gate.astype(jnp.float32))).astype(
        jnp.bfloat16
    )


def shards(
    tokens,
    norm_gain,
    conv_val_w,
    conv_gate_w,
    rec_gate_w,
    rec_in_w,
    conv_taps,
    conv_bias,
    conv_gain,
    short_taps,
    decay_map,
    input_map,
    decay_base,
    decay_jump,
    out_conv_w,
    out_rec_w,
):
    rec_cols = rec_in_w.shape[1]
    conv_lags = conv_taps.shape[0] - 1
    short_lags = short_taps.shape[0] - 1
    normed = norm_rows(tokens, norm_gain)
    val_full, gate_full = (
        lax.all_gather(conv_val_w, "sp", axis=0, tiled=True),
        lax.all_gather(conv_gate_w, "sp", axis=0, tiled=True),
    )
    all_rows = lax.all_gather(normed, "tp", axis=0, tiled=True)
    conv_val = jnp.dot(all_rows, val_full, preferred_element_type=jnp.float32).astype(jnp.bfloat16)
    conv_gate = jnp.dot(all_rows, gate_full, preferred_element_type=jnp.float32).astype(
        jnp.bfloat16
    )
    glu = glu_of(conv_val, conv_gate)
    conv_edge = passed_along(glu[-conv_lags:], "sp", 1)
    rgate_full, rin_full = (
        lax.all_gather(rec_gate_w, "sp", axis=0, tiled=True),
        lax.all_gather(rec_in_w, "sp", axis=0, tiled=True),
    )
    rec_gate = jnp.dot(all_rows, rgate_full, preferred_element_type=jnp.float32).astype(
        jnp.bfloat16
    )
    rec_in = jnp.dot(all_rows, rin_full, preferred_element_type=jnp.float32).astype(jnp.bfloat16)
    rec_edge = passed_along(rec_in[-short_lags:], "sp", 1)
    filtered = causal_window(conv_edge, glu, conv_taps) + conv_bias[None, :]
    row_total = lax.psum(jnp.sum(filtered, axis=1), "tp")
    centered = filtered - (row_total / CONV_WIDTH)[:, None]
    spread = lax.psum(jnp.sum(centered * centered, axis=1), "tp") / CONV_WIDTH
    conv_out = jax.nn.silu(centered * lax.rsqrt(spread + 1e-05)[:, None] * conv_gain).astype(
        jnp.bfloat16
    )
    smoothed = causal_window(rec_edge, rec_in, short_taps).astype(jnp.bfloat16)
    length = smoothed.shape[0]
    grouped = smoothed.reshape(length, decay_map.shape[0], decay_map.shape[1])
    retain = jax.nn.sigmoid(
        jnp.einsum("thi,hio->tho", grouped, decay_map, preferred_element_type=jnp.float32).reshape(
            length, rec_cols
        )
    )
    admit = jax.nn.sigmoid(
        jnp.einsum("thi,hio->tho", grouped, input_map, preferred_element_type=jnp.float32).reshape(
            length, rec_cols
        )
    )
    log_decay = -RATE_SCALE * retain * jax.nn.softplus(-decay_base)[None, :] + decay_jump
    decay = jnp.exp(log_decay)
    inflow = jnp.sqrt(-jnp.expm1(2.0 * log_decay)) * admit * smoothed.astype(jnp.float32)
    products, local_state = lax.associative_scan(chain_step, (decay, inflow), axis=0)
    entering = prefix(
        (products[-1], local_state[-1]),
        "sp",
        chain_step,
        (jnp.ones((rec_cols,), jnp.float32), jnp.zeros((rec_cols,), jnp.float32)),
    )
    state = local_state + products * entering[1][None, :]
    rec_out = (jax.nn.gelu(rec_gate.astype(jnp.float32)) * state).astype(jnp.bfloat16)
    conv_full, rec_full = (
        lax.all_gather(out_conv_w, "sp", axis=1, tiled=True),
        lax.all_gather(out_rec_w, "sp", axis=1, tiled=True),
    )
    return lax.psum_scatter(
        (
            jnp.dot(conv_out, conv_full, preferred_element_type=jnp.float32)
            + jnp.dot(rec_out, rec_full, preferred_element_type=jnp.float32)
        ).astype(jnp.bfloat16),
        "tp",
        scatter_dimension=0,
        tiled=True,
    )


MESH = pl.DeviceIdType.MESH
ANY = pl.BlockSpec(memory_space=pl.ANY)
VMEM = pl.BlockSpec(memory_space=pltpu.VMEM)
SEGMENTS = 8


class Spot:
    def __init__(self, planes):
        self.s, self.c = lax.axis_index("sp"), lax.axis_index("tp")
        self.z, self.q = self.s // 4, self.s % 4
        self.qx = self.q + 1 - 2 * (self.q % 2)
        self.qy = (self.q + 2) % 4
        self.qd = 3 - self.q
        self.has_up, self.has_down = self.z < planes - 1, self.z > 0
        self.up, self.down = self.at(self.s + 4, self.c), self.at(self.s - 4, self.c)
        self.partner = self.at(self.s, 1 - self.c)

    def at(self, s, c):
        return {"sp": s, "tp": c}

    def mate(self, q):
        return self.at(self.z * 4 + q, self.c)


class Mail:
    def __init__(self, send_sem):
        self.send_sem, self.count, self.open = send_sem, 0, []

    def send(self, src, dst, recv, device, when=None):
        copy = pltpu.make_async_remote_copy(
            src_ref=src, dst_ref=dst, send_sem=self.send_sem.at[self.count],
            recv_sem=recv, device_id=device, device_id_type=MESH,
        )
        self.count += 1
        self.open.append((copy.wait_send, when))
        if when is None:
            copy.start()
        else:
            pl.when(when)(copy.start)

    def local(self, src, dst):
        copy = pltpu.make_async_copy(src, dst, self.send_sem.at[self.count])
        self.count += 1
        copy.start()
        self.open.append((copy.wait, None))

    def arrived(self, dst, recv, device):
        pltpu.make_async_remote_copy(
            src_ref=dst, dst_ref=dst, send_sem=self.send_sem.at[0],
            recv_sem=recv, device_id=device, device_id_type=MESH,
        ).wait_recv()

    def finish(self):
        for wait, when in self.open:
            if when is None:
                wait()
            else:
                pl.when(when)(wait)


def greet(me, devices, line):
    barrier = pltpu.get_barrier_semaphore()
    for device in devices:
        pl.semaphore_signal(barrier, inc=1, device_id=device, device_id_type=MESH)
    amount = len(devices)
    if line:
        for has, device in ((me.has_up, me.up), (me.has_down, me.down)):
            @pl.when(has)
            def _():
                pl.semaphore_signal(barrier, inc=1, device_id=device, device_id_type=MESH)
        amount = amount + me.has_up.astype(jnp.int32) + me.has_down.astype(jnp.int32)
    pl.semaphore_wait(barrier, amount)


class PlaneGather:
    def __init__(self, me, mail, own, slot, recv, recv_pair):
        self.me, self.mail, self.own, self.slot = me, mail, own, slot
        self.recv, self.recv_pair = recv, recv_pair

    def start(self):
        me, mail = self.me, self.mail
        for h in (0, 1):
            for q, half in ((me.qx, h), (me.qy, 1 - h)):
                mail.send(self.own(half), self.slot(me.q, me.c, half), self.recv.at[me.q, half], me.mate(q))
        for half in (0, 1):
            mail.send(self.own(half), self.slot(me.q, me.c, half), self.recv_pair.at[me.q, half], me.partner)

    def took(self, q, half):
        me, mail = self.me, self.mail
        here = self.slot(q, me.c, half)
        mail.arrived(here, self.recv.at[q, half], me.partner)
        return here

    def share(self, q, half, here):
        self.mail.send(here, here, self.recv_pair.at[q, half], self.me.partner)

    def first(self):
        me = self.me
        for q, half, to in ((me.qx, 0, me.qy), (me.qy, 1, me.qx)):
            here = self.took(q, half)
            self.mail.send(here, here, self.recv.at[q, half], me.mate(to))
            self.share(q, half, here)

    def second(self):
        for q, half in ((self.me.qx, 1), (self.me.qy, 0)):
            self.share(q, half, self.took(q, half))

    def third(self):
        for half in (0, 1):
            self.share(self.me.qd, half, self.took(self.me.qd, half))

    def last(self):
        me = self.me
        for q in (me.q, me.qx, me.qy, me.qd):
            for half in (0, 1):
                self.mail.arrived(self.slot(q, 1 - me.c, half), self.recv_pair.at[q, half], me.partner)


def enter_kernel(
    planes, x_ref, gain, w_ref, j_ref, proj, jall, xall, wall, acc, send, rx, rp, rw, rz, rj
):
    me = Spot(planes)
    mail = Mail(send)
    greet(me, [me.mate(me.qx), me.mate(me.qy), me.mate(me.qd), me.partner], True)
    others = (me.qx, me.qy, me.qd)
    depth = w_ref.shape[1]
    rows = x_ref.shape[0]

    def wslot(origin, piece):
        return wall.at[pl.ds(pl.multiple_of((origin * 4 + piece) * depth, depth), depth)]

    def to_line(src, origin, piece):
        mail.send(src, wslot(origin, piece), rz.at[origin, piece], me.up, me.has_up)
        mail.send(src, wslot(origin, piece), rz.at[origin, piece], me.down, me.has_down)

    for q in others:
        mail.send(w_ref.at[q], wslot(me.z, me.q), rw.at[me.q], me.mate(q))
    to_line(w_ref.at[me.q], me.z, me.q)
    mail.local(w_ref.at[me.q], wslot(me.z, me.q))

    first_row = (me.q * 2 + me.c) * rows

    @pl.loop(0, rows // 16)
    def _(i):
        values = x_ref[pl.ds(pl.multiple_of(i * 16, 16), 16)].astype(jnp.float32)
        inverse = lax.rsqrt(jnp.mean(values * values, axis=1, keepdims=True) + 1e-06)
        place = pl.ds(pl.multiple_of(first_row + i * 16, 16), 16)
        xall[place] = (values * inverse * gain[...]).astype(xall.dtype)

    half_rows = rows // 2

    def slot(q, c, h):
        return xall.at[pl.ds(pl.multiple_of((q * 2 + c) * rows + h * half_rows, 16), half_rows)]

    xg = PlaneGather(me, mail, lambda h: slot(me.q, me.c, h), slot, rx, rp)
    xg.start()
    for q in others:
        mail.send(j_ref.at[q], jall.at[me.q], rj.at[me.q], me.mate(q))
    mail.local(j_ref.at[me.q], jall.at[me.q])
    for q in others:
        here = wslot(me.z, q)
        mail.arrived(here, rw.at[q], me.partner)
        to_line(here, me.z, q)

    def line_step(k):
        for piece in (me.q,) + others:
            for origin, there, on, more in (
                (me.z - k, me.z >= k, me.up, me.has_up),
                (me.z + k, me.z + k < planes, me.down, me.has_down),
            ):
                here = wslot(origin, piece)
                sem = rz.at[origin, piece]
                pl.when(there)(functools.partial(mail.arrived, here, sem, me.partner))
                mail.send(here, here, sem, on, jnp.logical_and(there, more))

    line_step(1)
    xg.first()
    for k in range(2, planes - 1):
        line_step(k)
    xg.second()
    for q in others:
        mail.arrived(jall.at[q], rj.at[q], me.partner)
    xg.third()
    xg.last()
    mail.finish()
    tile = acc.shape[0] // 4

    def multiply(start, size, fresh=False):
        at = pl.ds(pl.multiple_of(start, depth), size)

        @pl.loop(0, 4)
        def _(i):
            part = pl.ds(pl.multiple_of(i * tile, 16), tile)
            product = jnp.dot(xall[part, at], wall[at], preferred_element_type=jnp.float32)
            acc[part] = product if fresh else acc[part] + product

    multiply(me.z * 4 * depth, 4 * depth, True)
    for k in range(1, planes - 1):
        for origin, there in ((me.z - k, me.z >= k), (me.z + k, me.z + k < planes)):
            pl.when(there)(functools.partial(multiply, origin * 4 * depth, 4 * depth))
    far = planes - 1 - me.z

    @pl.when(jnp.logical_or(me.z == 0, me.z == planes - 1))
    def _():
        for piece in (me.q,) + others:
            mail.arrived(wslot(far, piece), rz.at[far, piece], me.partner)
            multiply((far * 4 + piece) * depth, depth)

    @pl.loop(0, 8)
    def _(i):
        part = pl.ds(pl.multiple_of(i * (tile // 2), 16), tile // 2)
        proj[part] = acc[part].astype(proj.dtype)


def enter(planes, tokens, gain, pieces, jumps):
    rows, width = tokens.shape
    depth, cols = pieces.shape[1:]
    dma, vmem = pltpu.SemaphoreType.DMA, pltpu.VMEM
    return pl.pallas_call(
        functools.partial(enter_kernel, planes),
        out_shape=(
            jax.ShapeDtypeStruct((8 * rows, cols), tokens.dtype),
            jax.ShapeDtypeStruct(jumps.shape, jumps.dtype),
        ),
        in_specs=[VMEM] * 4,
        out_specs=(VMEM,) * 2,
        scratch_shapes=[
            vmem((8 * rows, width), tokens.dtype),
            vmem((planes * 4 * depth, cols), pieces.dtype),
            vmem((8 * rows, cols), jnp.float32),
            dma((40 + 8 * planes,)), dma((4, 2)), dma((4, 2)), dma((4,)), dma((planes, 4)), dma((4,)),
        ],
        compiler_params=pltpu.CompilerParams(
            collective_id=0, has_side_effects=True, vmem_limit_bytes=56 * 1024 * 1024
        ),
    )(tokens, gain, pieces, jumps)


def minus_expm1(y):
    series = 1.0 + y * (1.0 / 8.0)
    for n in (7.0, 6.0, 5.0, 4.0, 3.0, 2.0):
        series = 1.0 + y * (1.0 / n) * series
    return jnp.where(y > -0.35, -y * series, 1.0 - jnp.exp(y))


def gelu(v):
    return 0.5 * v * (1.0 + jnp.tanh(0.7978845608028654 * (v + 0.044715 * v * v * v)))


def core_kernel(
    planes, lags, proj, jump, cpar, rpar, dmap, imap, w_ref,
    out, wz, wp, yall, cbuf, halo, gext, rext, filt, dec, inf, maps, stat, st_all, carry, cr_all,
    send, ry, rp, rv, rq, rz, rw, rh, rs, rc, ls, lr,
):
    me = Spot(planes)
    mail = Mail(send)
    c_lags, s_lags = lags
    f32, bf16 = jnp.float32, jnp.bfloat16
    length = proj.shape[0]
    cw = gext.shape[1]
    rwid = jump.shape[1]
    seg = length // SEGMENTS
    top = halo.shape[0]
    fold = dec.shape[0]
    part = planes // 2
    width = yall.shape[1] // 8
    mine = me.q * 2 + me.c
    mates = [me.at(me.z * 4 + (me.q + dq) % 4, c) for dq in range(4) for c in (me.c, 1 - me.c)][1:]
    lined = [me.at((me.s + 4 * k) % (4 * planes), me.c) for k in range(1, planes)]
    greet(me, mates + lined, False)

    def hand_over(src, origin, when):
        theirs = origin // part != me.c
        if when is not None:
            theirs = jnp.logical_and(theirs, when)
        place = origin - (1 - me.c) * part
        mail.send(src, wp.at[place], rw.at[place], me.partner, theirs)

    mail.send(proj.at[pl.ds(length - top, top)], halo, rh.at[0], me.up, me.has_up)
    mail.send(w_ref, wz.at[me.z], rz.at[me.z], me.up, me.has_up)
    mail.send(w_ref, wz.at[me.z], rz.at[me.z], me.down, me.has_down)
    hand_over(w_ref, me.z, None)
    mail.local(w_ref, wz.at[me.z])

    maps[...] = jnp.zeros_like(maps)
    size = dmap.shape[1]
    heads = rwid // size
    for h in range(heads):
        spot = pl.ds(h * size, size)
        maps[spot, pl.ds(h * size, size)] = dmap[me.q * heads + h]
        maps[spot, pl.ds(fold * 128 + h * size, size)] = imap[me.q * heads + h]

    def columns(ref, row, count):
        val = ref[pl.ds(row, count), pl.ds(0, cw)].astype(f32)
        gate = ref[pl.ds(row, count), pl.ds(cw, cw)].astype(f32)
        return (val * jax.nn.sigmoid(gate)).astype(bf16).astype(f32)

    rec_at, gate_at = 2 * cw + rwid, 2 * cw

    @pl.loop(0, SEGMENTS)
    def _(i):
        base = pl.multiple_of(i * seg, 16)
        rext[pl.ds(pl.multiple_of(base + top, 8), seg)] = proj[pl.ds(base, seg), pl.ds(rec_at, rwid)].astype(f32)

    @pl.when(me.has_down)
    def _():
        mail.arrived(halo, rh.at[0], me.partner)
        rext[pl.ds(0, top)] = halo[:, pl.ds(rec_at, rwid)].astype(f32)

    @pl.when(jnp.logical_not(me.has_down))
    def _():
        rext[pl.ds(0, top)] = jnp.zeros((top, rwid), f32)

    softened = rpar[me.q, pl.ds(s_lags + 1, 1), :]

    @pl.loop(0, SEGMENTS)
    def _(i):
        base = pl.multiple_of(i * seg, 8)
        window = rext[pl.ds(pl.multiple_of(base + top - 8, 8), seg + 8)]
        smooth = jnp.zeros((seg, rwid), f32)
        for k in range(s_lags + 1):
            smooth = smooth + rpar[me.q, pl.ds(k, 1), :] * window[8 - s_lags + k : 8 - s_lags + k + seg]
        smooth = smooth.astype(bf16)
        gates = jax.nn.sigmoid(jnp.dot(smooth, maps[...], preferred_element_type=f32))
        retain, admit = gates[:, :rwid], gates[:, fold * 128 : fold * 128 + rwid]
        log_decay = jump[pl.ds(base, seg)] - retain * softened
        decay = jnp.exp(log_decay)
        inflow = jnp.sqrt(minus_expm1(2.0 * log_decay)) * admit * smooth.astype(f32)
        for f in range(fold):
            w = min(128, rwid - f * 128)
            dec[f, pl.ds(base, seg), pl.ds(0, w)] = decay[:, f * 128 : f * 128 + w]
            inf[f, pl.ds(base, seg), pl.ds(0, w)] = inflow[:, f * 128 : f * 128 + w]

    def one(i, held):
        after = []
        for f in range(fold):
            at = pl.ds(i, SEGMENTS, stride=seg)
            d = dec.at[f][at, :]
            product, state = held[2 * f] * d, held[2 * f + 1] * d + inf.at[f][at, :]
            dec.at[f][at, :] = product
            inf.at[f][at, :] = state
            after += [product, state]
        return tuple(after)

    flat = (SEGMENTS, 128)
    ends = lax.fori_loop(0, seg, one, (jnp.ones(flat, f32), jnp.zeros(flat, f32)) * fold, unroll=8)
    for f in range(fold):
        product, state = jnp.ones((1, 128), f32), jnp.zeros((1, 128), f32)
        for i in range(SEGMENTS):
            p, s = ends[2 * f][i : i + 1], ends[2 * f + 1][i : i + 1]
            product, state = product * p, p * state + s
        carry[pl.ds(2 * f, 1)] = product
        carry[pl.ds(2 * f + 1, 1)] = state
    for device in lined:
        mail.send(carry, cr_all.at[me.z], rc.at[me.z], device)

    @pl.loop(0, SEGMENTS)
    def _(i):
        base = pl.multiple_of(i * seg, 16)
        gext[pl.ds(pl.multiple_of(base + top, 8), seg)] = columns(proj, base, seg)

    @pl.when(me.has_down)
    def _():
        gext[pl.ds(0, top)] = columns(halo, 0, top)

    @pl.when(jnp.logical_not(me.has_down))
    def _():
        gext[pl.ds(0, top)] = jnp.zeros((top, cw), f32)

    def line_step(k):
        for origin, there, on, more in (
            (me.z - k, me.z >= k, me.up, me.has_up),
            (me.z + k, me.z + k < planes, me.down, me.has_down),
        ):
            pl.when(there)(functools.partial(mail.arrived, wz.at[origin], rz.at[origin], me.partner))
            if k < planes - 1:
                mail.send(wz.at[origin], wz.at[origin], rz.at[origin], on, jnp.logical_and(there, more))
            hand_over(wz.at[origin], origin, there)

    for k in range(1, planes):
        z = (me.z + k) % planes
        mail.arrived(cr_all.at[z], rc.at[z], me.partner)
    cr_all[me.z] = carry[...]
    entering = []
    for f in range(fold):
        held = jnp.zeros((1, 128), f32)
        for j in range(planes - 1):
            after = cr_all[j, pl.ds(2 * f, 1)] * held + cr_all[j, pl.ds(2 * f + 1, 1)]
            held = jnp.where(j < me.z, after, held)
        for i in range(SEGMENTS):
            entering.append(held)
            held = ends[2 * f][i : i + 1] * held + ends[2 * f + 1][i : i + 1]
    own_at = pl.multiple_of(mine * width, 128)
    for i in range(SEGMENTS):
        rows = pl.ds(i * seg, seg)
        state = [dec[f, rows] * entering[f * SEGMENTS + i] + inf[f, rows] for f in range(fold)]
        state = jnp.concatenate(state, axis=1)[:, :rwid]
        result = gelu(proj[rows, pl.ds(gate_at, rwid)].astype(f32)) * state
        fill = jnp.zeros((seg, width - cw - rwid), f32)
        yall[rows, pl.ds(pl.multiple_of(own_at + cw, 128), width - cw)] = jnp.concatenate([result, fill], axis=1).astype(bf16)

    half_rows = length // 2

    def gather(lane, lanes, recv, recv_pair):
        def slot(q, c, h):
            spot = pl.ds(pl.multiple_of((q * 2 + c) * width + lane, 128), lanes)
            return yall.at[pl.ds(h * half_rows, half_rows), spot]

        return PlaneGather(me, mail, lambda h: slot(me.q, me.c, h), slot, recv, recv_pair)

    vg = gather(cw, width - cw, rv, rq)
    vg.start()

    @pl.loop(0, length // 64)
    def _(i):
        base = pl.multiple_of(i * 64, 8)
        window = gext[pl.ds(base, 64 + top)]
        total = jnp.zeros((64, cw), f32) + cpar[pl.ds(c_lags + 1, 1), :]
        for k in range(c_lags + 1):
            begin = top - c_lags + k
            total = total + cpar[pl.ds(k, 1), :] * window[begin : begin + 64]
        filt[pl.ds(base, 64)] = total
        part_sum = jnp.sum(total, axis=1, keepdims=True)
        off = total - part_sum * (1.0 / cw)
        lane = lax.broadcasted_iota(jnp.int32, (64, 128), 1)
        spread = jnp.sum(off * off, axis=1, keepdims=True)
        stat[pl.ds(base, 64)] = jnp.where(lane == 0, part_sum, spread)

    packed = stat[...].T
    st_all[mine] = packed[0:8]
    for device in mates:
        mail.send(st_all.at[mine], st_all.at[mine], rs.at[mine], device)

    line_step(1)
    for k in range(1, 8):
        d = (mine + k) % 8
        mail.arrived(st_all.at[d], rs.at[d], me.partner)
    total = sum(st_all[d, 0:1, :] for d in range(8))
    mean = total * (1.0 / (8 * cw))
    spread = jnp.zeros_like(mean)
    for d in range(8):
        shift = st_all[d, 0:1, :] * (1.0 / cw) - mean
        spread = spread + st_all[d, 1:2, :] + cw * shift * shift
    scale = lax.rsqrt(spread * (1.0 / (8 * cw)) + 1e-05)
    row = lax.broadcasted_iota(jnp.int32, (128, length), 0)
    stat[...] = jnp.where(row == 0, mean, scale).T

    @pl.loop(0, SEGMENTS)
    def _(i):
        rows = pl.ds(pl.multiple_of(i * seg, 16), seg)
        pair = stat[rows]
        v = (filt[rows] - pair[:, 0:1]) * pair[:, 1:2] * cpar[pl.ds(c_lags + 2, 1), :]
        yall[rows, pl.ds(own_at, cw)] = (v * jax.nn.sigmoid(v)).astype(bf16)

    yg = gather(0, cw, ry, rp)
    yg.start()
    vg.first()
    yg.first()
    for k in range(2, planes - 1):
        line_step(k)
    vg.second()
    yg.second()
    vg.third()
    yg.third()
    line_step(planes - 1)
    for k in range(part):
        mail.arrived(wp.at[k], rw.at[k], me.partner)
    vg.last()
    yg.last()
    mail.finish()

    used, cols = cw + rwid, w_ref.shape[1]
    tile = length // 8

    def multiply(d):
        rows = pl.ds(pl.multiple_of(d * tile, 16), tile)
        for k in range(part):
            total = jnp.zeros((tile, cols), f32)
            for q in range(4):
                for c, block in ((me.c, wz.at[me.c * part + k]), (1 - me.c, wp.at[k])):
                    left = yall[rows, pl.ds(pl.multiple_of((q * 2 + c) * width, 128), width)]
                    total = total + jnp.dot(
                        left[:, :used], block[pl.ds(q * used, used)], preferred_element_type=f32
                    )
            cbuf[d, k] = total.astype(bf16)

    def place(q, c, k):
        return out.at[:, pl.ds(pl.multiple_of(((c * part + k) * 4 + q) * cols, 128), cols)]

    def target(i):
        flip = 3 - i // 2
        q = (me.q // 2 + flip // 2) % 2 * 2 + (me.q % 2 + flip % 2) % 2
        return q, (me.c + 1 + i) % 2

    def parcel(i, k):
        q, c = target(i)
        return pltpu.make_async_remote_copy(
            src_ref=cbuf.at[q * 2 + c, k], dst_ref=place(me.q, me.c, k), send_sem=ls.at[i, k],
            recv_sem=lr.at[mine, k], device_id=me.at(me.z * 4 + q, c), device_id_type=MESH,
        )

    @pl.loop(0, 7)
    def _(i):
        q, c = target(i)
        multiply(q * 2 + c)
        for k in range(part):
            parcel(i, k).start()

    multiply(mine)
    kept = [pltpu.make_async_copy(cbuf.at[mine, k], place(me.q, me.c, k), ls.at[7, k]) for k in range(part)]
    for copy in kept:
        copy.start()

    @pl.loop(0, 7)
    def _(i):
        q, c = target(i)
        for k in range(part):
            mail.arrived(place(q, c, k), lr.at[q * 2 + c, k], me.partner)
            parcel(i, k).wait_send()

    for copy in kept:
        copy.wait()


def core(planes, proj, jump, cpar, rpar, dmap, imap, weights, lags, cw):
    length, rwid = jump.shape
    used, cols = cw + rwid, weights.shape[1]
    width = used + -used % 128
    fold = (rwid + 127) // 128
    f32, bf16 = jnp.float32, jnp.bfloat16
    dma, vmem = pltpu.SemaphoreType.DMA, pltpu.VMEM
    top = lags[0] + -lags[0] % 16
    part = planes // 2
    return pl.pallas_call(
        functools.partial(core_kernel, planes, lags),
        out_shape=jax.ShapeDtypeStruct((length // 8, planes * 4 * cols), bf16),
        in_specs=[VMEM] * 7,
        out_specs=ANY,
        scratch_shapes=[
            vmem((planes,) + weights.shape, bf16),
            vmem((part,) + weights.shape, bf16),
            vmem((length, 8 * width), bf16),
            vmem((8, part, length // 8, cols), bf16),
            vmem((top, proj.shape[1]), bf16),
            vmem((top + length, cw), f32),
            vmem((top + length, rwid), f32),
            vmem((length, cw), f32),
            vmem((fold, length, 128), f32),
            vmem((fold, length, 128), f32),
            vmem((rwid, 2 * fold * 128), bf16),
            vmem((length, 128), f32),
            vmem((8, 8, length), f32),
            vmem((8, 128), f32),
            vmem((planes, 8, 128), f32),
            dma((64 + 8 * planes,)), dma((4, 2)), dma((4, 2)), dma((4, 2)), dma((4, 2)), dma((planes,)), dma((part,)),
            dma((1,)), dma((8,)), dma((planes,)), dma((8, part)), dma((8, part)),
        ],
        compiler_params=pltpu.CompilerParams(
            collective_id=2, has_side_effects=True, vmem_limit_bytes=60 * 1024 * 1024
        ),
    )(proj, jump, cpar, rpar, dmap, imap, weights)


def plane_shards(
    planes,
    tokens,
    norm_gain,
    conv_val_w,
    conv_gate_w,
    rec_gate_w,
    rec_in_w,
    conv_taps,
    conv_bias,
    conv_gain,
    short_taps,
    decay_map,
    input_map,
    decay_base,
    decay_jump,
    out_conv_w,
    out_rec_w,
):
    s = lax.axis_index("sp")
    q = s % 4
    f32 = jnp.float32

    def by_mate(a):
        return a.reshape(a.shape[0], 4, a.shape[1] // 4).transpose(1, 0, 2)

    def mine(a, axis):
        size = a.shape[axis] // 4
        return lax.dynamic_slice_in_dim(a, q * size, size, axis)

    pieces = jnp.concatenate([by_mate(w) for w in (conv_val_w, conv_gate_w, rec_gate_w, rec_in_w)], axis=2)
    projected, jall = enter(planes, tokens, norm_gain[None], pieces, by_mate(decay_jump))
    cw, rw = conv_val_w.shape[1] // 4, rec_in_w.shape[1] // 4
    jump = jall.reshape(-1, rw)
    cols = out_conv_w.shape[1]
    rows_by_mate = jnp.concatenate(
        [out_conv_w.reshape(4, cw, cols), out_rec_w.reshape(4, rw, cols)], axis=1
    ).reshape(-1, cols)
    cpar = mine(jnp.concatenate([conv_taps.astype(f32), conv_bias[None], conv_gain[None]]), 1)
    rpar = by_mate(jnp.concatenate([short_taps.astype(f32), RATE_SCALE * jax.nn.softplus(-decay_base)[None]]))
    lags = (conv_taps.shape[0] - 1, short_taps.shape[0] - 1)
    return core(planes, projected, jump, cpar, rpar, decay_map, input_map, rows_by_mate, lags, cw)


def solution(mesh):
    in_specs = (
        P(("sp", "tp"), None),
        P(),
        P("sp", "tp"),
        P("sp", "tp"),
        P("sp", "tp"),
        P("sp", "tp"),
        P(None, "tp"),
        P("tp"),
        P("tp"),
        P(None, "tp"),
        P("tp", None, None),
        P("tp", None, None),
        P("tp"),
        P("sp", "tp"),
        P("tp", "sp"),
        P("tp", "sp"),
    )
    out_specs = P(("sp", "tp"), None)
    count = mesh.shape["sp"]
    planar = mesh.shape["tp"] == 2 and count % 8 == 0 and count >= 16
    body = functools.partial(plane_shards, count // 4) if planar else shards
    return jax.shard_map(body, mesh=mesh, in_specs=in_specs, out_specs=out_specs, check_vma=False)
```

```python
import functools

import jax
import jax.numpy as jnp
from jax import lax
from jax.experimental import pallas as pl
from jax.experimental.pallas import tpu as pltpu
from jax.sharding import PartitionSpec as P

CONV_WIDTH = 1024


RATE_SCALE = 8.0


def passed_along(value, axis, by):
    count = lax.axis_size(axis)
    pairs = [(i, i + by) for i in range(count) if 0 <= i + by < count]
    return lax.ppermute(value, axis, pairs)


def prefix(part, axis, combine, identity):
    place = lax.axis_index(axis)
    gathered = jax.tree.map(lambda a: lax.all_gather(a, axis), part)
    state = jax.tree.map(lambda a, e: jnp.zeros_like(a) + jnp.asarray(e, a.dtype), part, identity)

    def one(step, state):
        return combine(
            state, jax.tree.map(lambda a: lax.dynamic_index_in_dim(a, step, 0, False), gathered)
        )

    return lax.fori_loop(0, place, one, state)


def norm_rows(values, gain):
    widened = values.astype(jnp.float32)
    inverse = lax.rsqrt(jnp.mean(widened * widened, axis=-1, keepdims=True) + 1e-06)
    return (widened * inverse * gain).astype(jnp.bfloat16)


def causal_window(edge, current, weights):
    extended = jnp.concatenate([edge, current], axis=0).astype(jnp.float32)
    taps_wide = weights.astype(jnp.float32)
    length = current.shape[0]
    result = jnp.zeros((length, current.shape[1]), jnp.float32)
    for lag_index in range(weights.shape[0]):
        result = result + taps_wide[lag_index][None, :] * extended[lag_index : lag_index + length]
    return result


def chain_step(earlier, latter):
    return (earlier[0] * latter[0], latter[0] * earlier[1] + latter[1])


def glu_of(conv_val, conv_gate):
    return (conv_val.astype(jnp.float32) * jax.nn.sigmoid(conv_gate.astype(jnp.float32))).astype(
        jnp.bfloat16
    )


def shards(
    tokens,
    norm_gain,
    conv_val_w,
    conv_gate_w,
    rec_gate_w,
    rec_in_w,
    conv_taps,
    conv_bias,
    conv_gain,
    short_taps,
    decay_map,
    input_map,
    decay_base,
    decay_jump,
    out_conv_w,
    out_rec_w,
):
    rec_cols = rec_in_w.shape[1]
    conv_lags = conv_taps.shape[0] - 1
    short_lags = short_taps.shape[0] - 1
    normed = norm_rows(tokens, norm_gain)
    val_full, gate_full = (
        lax.all_gather(conv_val_w, "sp", axis=0, tiled=True),
        lax.all_gather(conv_gate_w, "sp", axis=0, tiled=True),
    )
    all_rows = lax.all_gather(normed, "tp", axis=0, tiled=True)
    conv_val = jnp.dot(all_rows, val_full, preferred_element_type=jnp.float32).astype(jnp.bfloat16)
    conv_gate = jnp.dot(all_rows, gate_full, preferred_element_type=jnp.float32).astype(
        jnp.bfloat16
    )
    glu = glu_of(conv_val, conv_gate)
    conv_edge = passed_along(glu[-conv_lags:], "sp", 1)
    rgate_full, rin_full = (
        lax.all_gather(rec_gate_w, "sp", axis=0, tiled=True),
        lax.all_gather(rec_in_w, "sp", axis=0, tiled=True),
    )
    rec_gate = jnp.dot(all_rows, rgate_full, preferred_element_type=jnp.float32).astype(
        jnp.bfloat16
    )
    rec_in = jnp.dot(all_rows, rin_full, preferred_element_type=jnp.float32).astype(jnp.bfloat16)
    rec_edge = passed_along(rec_in[-short_lags:], "sp", 1)
    filtered = causal_window(conv_edge, glu, conv_taps) + conv_bias[None, :]
    row_total = lax.psum(jnp.sum(filtered, axis=1), "tp")
    centered = filtered - (row_total / CONV_WIDTH)[:, None]
    spread = lax.psum(jnp.sum(centered * centered, axis=1), "tp") / CONV_WIDTH
    conv_out = jax.nn.silu(centered * lax.rsqrt(spread + 1e-05)[:, None] * conv_gain).astype(
        jnp.bfloat16
    )
    smoothed = causal_window(rec_edge, rec_in, short_taps).astype(jnp.bfloat16)
    length = smoothed.shape[0]
    grouped = smoothed.reshape(length, decay_map.shape[0], decay_map.shape[1])
    retain = jax.nn.sigmoid(
        jnp.einsum("thi,hio->tho", grouped, decay_map, preferred_element_type=jnp.float32).reshape(
            length, rec_cols
        )
    )
    admit = jax.nn.sigmoid(
        jnp.einsum("thi,hio->tho", grouped, input_map, preferred_element_type=jnp.float32).reshape(
            length, rec_cols
        )
    )
    log_decay = -RATE_SCALE * retain * jax.nn.softplus(-decay_base)[None, :] + decay_jump
    decay = jnp.exp(log_decay)
    inflow = jnp.sqrt(-jnp.expm1(2.0 * log_decay)) * admit * smoothed.astype(jnp.float32)
    products, local_state = lax.associative_scan(chain_step, (decay, inflow), axis=0)
    entering = prefix(
        (products[-1], local_state[-1]),
        "sp",
        chain_step,
        (jnp.ones((rec_cols,), jnp.float32), jnp.zeros((rec_cols,), jnp.float32)),
    )
    state = local_state + products * entering[1][None, :]
    rec_out = (jax.nn.gelu(rec_gate.astype(jnp.float32)) * state).astype(jnp.bfloat16)
    conv_full, rec_full = (
        lax.all_gather(out_conv_w, "sp", axis=1, tiled=True),
        lax.all_gather(out_rec_w, "sp", axis=1, tiled=True),
    )
    return lax.psum_scatter(
        (
            jnp.dot(conv_out, conv_full, preferred_element_type=jnp.float32)
            + jnp.dot(rec_out, rec_full, preferred_element_type=jnp.float32)
        ).astype(jnp.bfloat16),
        "tp",
        scatter_dimension=0,
        tiled=True,
    )


MESH = pl.DeviceIdType.MESH
ANY = pl.BlockSpec(memory_space=pl.ANY)
VMEM = pl.BlockSpec(memory_space=pltpu.VMEM)
SEGMENTS = 8


class Spot:
    def __init__(self, planes):
        self.s, self.c = lax.axis_index("sp"), lax.axis_index("tp")
        self.z, self.q = self.s // 4, self.s % 4
        self.qx = self.q + 1 - 2 * (self.q % 2)
        self.qy = (self.q + 2) % 4
        self.qd = 3 - self.q
        self.has_up, self.has_down = self.z < planes - 1, self.z > 0
        self.up, self.down = self.at(self.s + 4, self.c), self.at(self.s - 4, self.c)
        self.partner = self.at(self.s, 1 - self.c)

    def at(self, s, c):
        return {"sp": s, "tp": c}

    def mate(self, q):
        return self.at(self.z * 4 + q, self.c)


class Mail:
    def __init__(self, send_sem):
        self.send_sem, self.count, self.open = send_sem, 0, []

    def send(self, src, dst, recv, device, when=None):
        copy = pltpu.make_async_remote_copy(
            src_ref=src, dst_ref=dst, send_sem=self.send_sem.at[self.count],
            recv_sem=recv, device_id=device, device_id_type=MESH,
        )
        self.count += 1
        self.open.append((copy.wait_send, when))
        if when is None:
            copy.start()
        else:
            pl.when(when)(copy.start)

    def local(self, src, dst):
        copy = pltpu.make_async_copy(src, dst, self.send_sem.at[self.count])
        self.count += 1
        copy.start()
        self.open.append((copy.wait, None))
        return self.open[-1]

    def arrived(self, dst, recv, device):
        pltpu.make_async_remote_copy(
            src_ref=dst, dst_ref=dst, send_sem=self.send_sem.at[0],
            recv_sem=recv, device_id=device, device_id_type=MESH,
        ).wait_recv()

    def finish(self):
        for wait, when in self.open:
            if when is None:
                wait()
            else:
                pl.when(when)(wait)


def greet(me, devices, line):
    barrier = pltpu.get_barrier_semaphore()
    for device in devices:
        pl.semaphore_signal(barrier, inc=1, device_id=device, device_id_type=MESH)
    amount = len(devices)
    if line:
        for has, device in ((me.has_up, me.up), (me.has_down, me.down)):
            @pl.when(has)
            def _():
                pl.semaphore_signal(barrier, inc=1, device_id=device, device_id_type=MESH)
        amount = amount + me.has_up.astype(jnp.int32) + me.has_down.astype(jnp.int32)
    pl.semaphore_wait(barrier, amount)


class PlaneGather:
    def __init__(self, me, mail, own, slot, recv, recv_pair):
        self.me, self.mail, self.own, self.slot = me, mail, own, slot
        self.recv, self.recv_pair = recv, recv_pair

    def start(self):
        me, mail = self.me, self.mail
        for h in (0, 1):
            for q, half in ((me.qx, h), (me.qy, 1 - h)):
                mail.send(self.own(half), self.slot(me.q, me.c, half), self.recv.at[me.q, half], me.mate(q))
        for half in (0, 1):
            mail.send(self.own(half), self.slot(me.q, me.c, half), self.recv_pair.at[me.q, half], me.partner)

    def took(self, q, half):
        me, mail = self.me, self.mail
        here = self.slot(q, me.c, half)
        mail.arrived(here, self.recv.at[q, half], me.partner)
        return here

    def share(self, q, half, here):
        self.mail.send(here, here, self.recv_pair.at[q, half], self.me.partner)

    def first(self):
        me = self.me
        for q, half, to in ((me.qx, 0, me.qy), (me.qy, 1, me.qx)):
            here = self.took(q, half)
            self.mail.send(here, here, self.recv.at[q, half], me.mate(to))
            self.share(q, half, here)

    def second(self):
        for q, half in ((self.me.qx, 1), (self.me.qy, 0)):
            self.share(q, half, self.took(q, half))

    def third(self):
        for half in (0, 1):
            self.share(self.me.qd, half, self.took(self.me.qd, half))

    def last(self):
        me = self.me
        for q in (me.q, me.qx, me.qy, me.qd):
            for half in (0, 1):
                self.mail.arrived(self.slot(q, 1 - me.c, half), self.recv_pair.at[q, half], me.partner)


def enter_kernel(
    planes, x_ref, gain, w_ref, j_ref, proj, jall, xall, wall, acc, send, rx, rp, rw, rz, rj
):
    me = Spot(planes)
    mail = Mail(send)
    greet(me, [me.mate(me.qx), me.mate(me.qy), me.mate(me.qd), me.partner], True)
    others = (me.qx, me.qy, me.qd)
    depth = w_ref.shape[1]
    rows = x_ref.shape[0]
    jwidth = j_ref.shape[1] // 4

    def wslot(origin, piece):
        return wall.at[pl.ds(pl.multiple_of((origin * 4 + piece) * depth, depth), depth)]

    def to_line(src, origin, piece):
        mail.send(src, wslot(origin, piece), rz.at[origin, piece], me.up, me.has_up)
        mail.send(src, wslot(origin, piece), rz.at[origin, piece], me.down, me.has_down)

    for q in others:
        mail.send(w_ref.at[q], wslot(me.z, me.q), rw.at[me.q], me.mate(q))
    to_line(w_ref.at[me.q], me.z, me.q)
    own_rows = mail.local(w_ref.at[me.q], wslot(me.z, me.q))

    first_row = (me.q * 2 + me.c) * rows

    @pl.loop(0, rows // 16)
    def _(i):
        values = x_ref[pl.ds(pl.multiple_of(i * 16, 16), 16)].astype(jnp.float32)
        inverse = lax.rsqrt(jnp.mean(values * values, axis=1, keepdims=True) + 1e-06)
        place = pl.ds(pl.multiple_of(first_row + i * 16, 16), 16)
        xall[place] = (values * inverse * gain[...]).astype(xall.dtype)

    half_rows = rows // 2

    def slot(q, c, h):
        return xall.at[pl.ds(pl.multiple_of((q * 2 + c) * rows + h * half_rows, 16), half_rows)]

    xg = PlaneGather(me, mail, lambda h: slot(me.q, me.c, h), slot, rx, rp)
    xg.start()
    for q in others:
        here = wslot(me.z, q)
        mail.arrived(here, rw.at[q], me.partner)
        to_line(here, me.z, q)

    def line_step(k):
        for piece in (me.q,) + others:
            for origin, there, on, more in (
                (me.z - k, me.z >= k, me.up, me.has_up),
                (me.z + k, me.z + k < planes, me.down, me.has_down),
            ):
                here = wslot(origin, piece)
                sem = rz.at[origin, piece]
                pl.when(there)(functools.partial(mail.arrived, here, sem, me.partner))
                mail.send(here, here, sem, on, jnp.logical_and(there, more))

    line_step(1)
    xg.first()

    def share(q):
        begin = q * jwidth // 128 * 128
        return j_ref.at[:, pl.ds(pl.multiple_of(begin, 128), jall.shape[2])]

    for q in others:
        mail.send(share(q), jall.at[me.q], rj.at[me.q], me.mate(q))
    mail.local(share(me.q), jall.at[me.q])
    for k in range(2, planes - 1):
        line_step(k)
    xg.second()
    xg.third()
    xg.last()
    mail.open.remove(own_rows)
    own_rows[0]()
    tile = acc.shape[0] // 4

    def multiply(start, size, fresh=False):
        at = pl.ds(pl.multiple_of(start, depth), size)

        @pl.loop(0, 4)
        def _(i):
            part = pl.ds(pl.multiple_of(i * tile, 16), tile)
            product = jnp.dot(xall[part, at], wall[at], preferred_element_type=jnp.float32)
            acc[part] = product if fresh else acc[part] + product

    multiply(me.z * 4 * depth, 4 * depth, True)
    for k in range(1, planes - 1):
        for origin, there in ((me.z - k, me.z >= k), (me.z + k, me.z + k < planes)):
            pl.when(there)(functools.partial(multiply, origin * 4 * depth, 4 * depth))
    far = planes - 1 - me.z

    @pl.when(jnp.logical_or(me.z == 0, me.z == planes - 1))
    def _():
        for piece in (me.q,) + others:
            mail.arrived(wslot(far, piece), rz.at[far, piece], me.partner)
            multiply((far * 4 + piece) * depth, depth)

    for q in others:
        mail.arrived(jall.at[q], rj.at[q], me.partner)
    mail.finish()

    @pl.loop(0, 8)
    def _(i):
        part = pl.ds(pl.multiple_of(i * (tile // 2), 16), tile // 2)
        proj[part] = acc[part].astype(proj.dtype)


def window_of(width):
    return max(-(-(q + 1) * width // 128) * 128 - q * width // 128 * 128 for q in range(4))


def enter(planes, tokens, gain, pieces, jumps):
    rows, width = tokens.shape
    depth, cols = pieces.shape[1:]
    dma, vmem = pltpu.SemaphoreType.DMA, pltpu.VMEM
    return pl.pallas_call(
        functools.partial(enter_kernel, planes),
        out_shape=(
            jax.ShapeDtypeStruct((8 * rows, cols), tokens.dtype),
            jax.ShapeDtypeStruct((4, jumps.shape[0], window_of(jumps.shape[1] // 4)), jumps.dtype),
        ),
        in_specs=[VMEM] * 4,
        out_specs=(VMEM,) * 2,
        scratch_shapes=[
            vmem((8 * rows, width), tokens.dtype),
            vmem((planes * 4 * depth, cols), pieces.dtype),
            vmem((8 * rows, cols), jnp.float32),
            dma((40 + 8 * planes,)), dma((4, 2)), dma((4, 2)), dma((4,)), dma((planes, 4)), dma((4,)),
        ],
        compiler_params=pltpu.CompilerParams(
            collective_id=0, has_side_effects=True, vmem_limit_bytes=56 * 1024 * 1024
        ),
    )(tokens, gain, pieces, jumps)


def minus_expm1(y):
    series = 1.0 + y * (1.0 / 8.0)
    for n in (7.0, 6.0, 5.0, 4.0, 3.0, 2.0):
        series = 1.0 + y * (1.0 / n) * series
    return jnp.where(y > -0.35, -y * series, 1.0 - jnp.exp(y))


def gelu(v):
    return 0.5 * v * (1.0 + jnp.tanh(0.7978845608028654 * (v + 0.044715 * v * v * v)))


def core_kernel(
    planes, lags, proj, jump, cpar, rpar, dmap, imap, w_ref,
    out, wz, wp, yall, cbuf, halo, gext, rext, filt, dec, inf, maps, stat, st_all, carry, cr_all,
    send, ry, rp, rv, rq, rz, rw, rh, rs, rc, ls, lr,
):
    me = Spot(planes)
    mail = Mail(send)
    c_lags, s_lags = lags
    f32, bf16 = jnp.float32, jnp.bfloat16
    length = proj.shape[0]
    cw = gext.shape[1]
    rwid = rpar.shape[2]
    seg = length // SEGMENTS
    top = halo.shape[0]
    fold = dec.shape[0]
    part = planes // 2
    width = yall.shape[1] // 8
    mine = me.q * 2 + me.c
    mates = [me.at(me.z * 4 + (me.q + dq) % 4, c) for dq in range(4) for c in (me.c, 1 - me.c)][1:]
    lined = [me.at((me.s + 4 * k) % (4 * planes), me.c) for k in range(1, planes)]
    greet(me, mates + lined, False)

    def hand_over(src, origin, when):
        theirs = origin // part != me.c
        if when is not None:
            theirs = jnp.logical_and(theirs, when)
        place = origin - (1 - me.c) * part
        mail.send(src, wp.at[place], rw.at[place], me.partner, theirs)

    mail.send(proj.at[pl.ds(length - top, top)], halo, rh.at[0], me.up, me.has_up)
    mail.send(w_ref, wz.at[me.z], rz.at[me.z], me.up, me.has_up)
    mail.send(w_ref, wz.at[me.z], rz.at[me.z], me.down, me.has_down)
    hand_over(w_ref, me.z, None)
    mail.local(w_ref, wz.at[me.z])

    maps[...] = jnp.zeros_like(maps)
    size = dmap.shape[1]
    heads = rwid // size
    for h in range(heads):
        spot = pl.ds(h * size, size)
        maps[spot, pl.ds(h * size, size)] = dmap[me.q * heads + h]
        maps[spot, pl.ds(fold * 128 + h * size, size)] = imap[me.q * heads + h]

    def columns(ref, row, count):
        val = ref[pl.ds(row, count), pl.ds(0, cw)].astype(f32)
        gate = ref[pl.ds(row, count), pl.ds(cw, cw)].astype(f32)
        return (val * jax.nn.sigmoid(gate)).astype(bf16).astype(f32)

    rec_at, gate_at = 2 * cw + rwid, 2 * cw

    @pl.loop(0, SEGMENTS)
    def _(i):
        base = pl.multiple_of(i * seg, 16)
        rext[pl.ds(pl.multiple_of(base + top, 8), seg)] = proj[pl.ds(base, seg), pl.ds(rec_at, rwid)].astype(f32)

    @pl.when(me.has_down)
    def _():
        mail.arrived(halo, rh.at[0], me.partner)
        rext[pl.ds(0, top)] = halo[:, pl.ds(rec_at, rwid)].astype(f32)

    @pl.when(jnp.logical_not(me.has_down))
    def _():
        rext[pl.ds(0, top)] = jnp.zeros((top, rwid), f32)

    softened = rpar[me.q, pl.ds(s_lags + 1, 1), :]

    @pl.loop(0, SEGMENTS)
    def _(i):
        base = pl.multiple_of(i * seg, 8)
        window = rext[pl.ds(pl.multiple_of(base + top - 8, 8), seg + 8)]
        smooth = jnp.zeros((seg, rwid), f32)
        for k in range(s_lags + 1):
            smooth = smooth + rpar[me.q, pl.ds(k, 1), :] * window[8 - s_lags + k : 8 - s_lags + k + seg]
        smooth = smooth.astype(bf16)
        gates = jax.nn.sigmoid(jnp.dot(smooth, maps[...], preferred_element_type=f32))
        retain, admit = gates[:, :rwid], gates[:, fold * 128 : fold * 128 + rwid]
        wide = jump[pl.ds(base, seg)]
        moved = wide[:, :rwid]
        for lead in {q * rwid % 128 for q in range(4)} - {0}:
            moved = jnp.where(me.q * rwid % 128 == lead, wide[:, lead : lead + rwid], moved)
        log_decay = moved - retain * softened
        decay = jnp.exp(log_decay)
        inflow = jnp.sqrt(minus_expm1(2.0 * log_decay)) * admit * smooth.astype(f32)
        for f in range(fold):
            w = min(128, rwid - f * 128)
            dec[f, pl.ds(base, seg), pl.ds(0, w)] = decay[:, f * 128 : f * 128 + w]
            inf[f, pl.ds(base, seg), pl.ds(0, w)] = inflow[:, f * 128 : f * 128 + w]

    def one(i, held):
        after = []
        for f in range(fold):
            at = pl.ds(i, SEGMENTS, stride=seg)
            d = dec.at[f][at, :]
            product, state = held[2 * f] * d, held[2 * f + 1] * d + inf.at[f][at, :]
            dec.at[f][at, :] = product
            inf.at[f][at, :] = state
            after += [product, state]
        return tuple(after)

    flat = (SEGMENTS, 128)
    ends = lax.fori_loop(0, seg, one, (jnp.ones(flat, f32), jnp.zeros(flat, f32)) * fold, unroll=8)
    for f in range(fold):
        product, state = jnp.ones((1, 128), f32), jnp.zeros((1, 128), f32)
        for i in range(SEGMENTS):
            p, s = ends[2 * f][i : i + 1], ends[2 * f + 1][i : i + 1]
            product, state = product * p, p * state + s
        carry[pl.ds(2 * f, 1)] = product
        carry[pl.ds(2 * f + 1, 1)] = state
    for device in lined:
        mail.send(carry, cr_all.at[me.z], rc.at[me.z], device)

    @pl.loop(0, SEGMENTS)
    def _(i):
        base = pl.multiple_of(i * seg, 16)
        gext[pl.ds(pl.multiple_of(base + top, 8), seg)] = columns(proj, base, seg)

    @pl.when(me.has_down)
    def _():
        gext[pl.ds(0, top)] = columns(halo, 0, top)

    @pl.when(jnp.logical_not(me.has_down))
    def _():
        gext[pl.ds(0, top)] = jnp.zeros((top, cw), f32)

    def line_step(k):
        for origin, there, on, more in (
            (me.z - k, me.z >= k, me.up, me.has_up),
            (me.z + k, me.z + k < planes, me.down, me.has_down),
        ):
            pl.when(there)(functools.partial(mail.arrived, wz.at[origin], rz.at[origin], me.partner))
            if k < planes - 1:
                mail.send(wz.at[origin], wz.at[origin], rz.at[origin], on, jnp.logical_and(there, more))
            hand_over(wz.at[origin], origin, there)

    for k in range(1, planes):
        z = (me.z + k) % planes
        mail.arrived(cr_all.at[z], rc.at[z], me.partner)
    cr_all[me.z] = carry[...]
    entering = []
    for f in range(fold):
        held = jnp.zeros((1, 128), f32)
        for j in range(planes - 1):
            after = cr_all[j, pl.ds(2 * f, 1)] * held + cr_all[j, pl.ds(2 * f + 1, 1)]
            held = jnp.where(j < me.z, after, held)
        for i in range(SEGMENTS):
            entering.append(held)
            held = ends[2 * f][i : i + 1] * held + ends[2 * f + 1][i : i + 1]
    own_at = pl.multiple_of(mine * width, 128)
    for i in range(SEGMENTS):
        rows = pl.ds(i * seg, seg)
        state = [dec[f, rows] * entering[f * SEGMENTS + i] + inf[f, rows] for f in range(fold)]
        state = jnp.concatenate(state, axis=1)[:, :rwid]
        result = gelu(proj[rows, pl.ds(gate_at, rwid)].astype(f32)) * state
        fill = jnp.zeros((seg, width - cw - rwid), f32)
        yall[rows, pl.ds(pl.multiple_of(own_at + cw, 128), width - cw)] = jnp.concatenate([result, fill], axis=1).astype(bf16)

    half_rows = length // 2

    def gather(lane, lanes, recv, recv_pair):
        def slot(q, c, h):
            spot = pl.ds(pl.multiple_of((q * 2 + c) * width + lane, 128), lanes)
            return yall.at[pl.ds(h * half_rows, half_rows), spot]

        return PlaneGather(me, mail, lambda h: slot(me.q, me.c, h), slot, recv, recv_pair)

    vg = gather(cw, width - cw, rv, rq)
    vg.start()

    @pl.loop(0, length // 64)
    def _(i):
        base = pl.multiple_of(i * 64, 8)
        window = gext[pl.ds(base, 64 + top)]
        total = jnp.zeros((64, cw), f32) + cpar[pl.ds(c_lags + 1, 1), :]
        for k in range(c_lags + 1):
            begin = top - c_lags + k
            total = total + cpar[pl.ds(k, 1), :] * window[begin : begin + 64]
        filt[pl.ds(base, 64)] = total
        part_sum = jnp.sum(total, axis=1, keepdims=True)
        off = total - part_sum * (1.0 / cw)
        lane = lax.broadcasted_iota(jnp.int32, (64, 128), 1)
        spread = jnp.sum(off * off, axis=1, keepdims=True)
        stat[pl.ds(base, 64)] = jnp.where(lane == 0, part_sum, spread)

    packed = stat[...].T
    st_all[mine] = packed[0:8]
    for device in mates:
        mail.send(st_all.at[mine], st_all.at[mine], rs.at[mine], device)

    line_step(1)
    for k in range(1, 8):
        d = (mine + k) % 8
        mail.arrived(st_all.at[d], rs.at[d], me.partner)
    total = sum(st_all[d, 0:1, :] for d in range(8))
    mean = total * (1.0 / (8 * cw))
    spread = jnp.zeros_like(mean)
    for d in range(8):
        shift = st_all[d, 0:1, :] * (1.0 / cw) - mean
        spread = spread + st_all[d, 1:2, :] + cw * shift * shift
    scale = lax.rsqrt(spread * (1.0 / (8 * cw)) + 1e-05)
    row = lax.broadcasted_iota(jnp.int32, (128, length), 0)
    stat[...] = jnp.where(row == 0, mean, scale).T

    @pl.loop(0, SEGMENTS)
    def _(i):
        rows = pl.ds(pl.multiple_of(i * seg, 16), seg)
        pair = stat[rows]
        v = (filt[rows] - pair[:, 0:1]) * pair[:, 1:2] * cpar[pl.ds(c_lags + 2, 1), :]
        yall[rows, pl.ds(own_at, cw)] = (v * jax.nn.sigmoid(v)).astype(bf16)

    yg = gather(0, cw, ry, rp)
    yg.start()
    vg.first()
    yg.first()
    for k in range(2, planes - 1):
        line_step(k)
    vg.second()
    yg.second()
    vg.third()
    yg.third()
    line_step(planes - 1)
    for k in range(part):
        mail.arrived(wp.at[k], rw.at[k], me.partner)
    vg.last()
    yg.last()
    mail.finish()

    used, cols = cw + rwid, w_ref.shape[1]
    tile = length // 8

    def multiply(d):
        rows = pl.ds(pl.multiple_of(d * tile, 16), tile)
        for k in range(part):
            total = jnp.zeros((tile, cols), f32)
            for q in range(4):
                for c, block in ((me.c, wz.at[me.c * part + k]), (1 - me.c, wp.at[k])):
                    left = yall[rows, pl.ds(pl.multiple_of((q * 2 + c) * width, 128), width)]
                    total = total + jnp.dot(
                        left[:, :used], block[pl.ds(q * used, used)], preferred_element_type=f32
                    )
            cbuf[d, k] = total.astype(bf16)

    def place(q, c, k):
        return out.at[:, pl.ds(pl.multiple_of(((c * part + k) * 4 + q) * cols, 128), cols)]

    def target(i):
        flip = 3 - i // 2
        q = (me.q // 2 + flip // 2) % 2 * 2 + (me.q % 2 + flip % 2) % 2
        return q, (me.c + 1 + i) % 2

    def parcel(i, k):
        q, c = target(i)
        return pltpu.make_async_remote_copy(
            src_ref=cbuf.at[q * 2 + c, k], dst_ref=place(me.q, me.c, k), send_sem=ls.at[i, k],
            recv_sem=lr.at[mine, k], device_id=me.at(me.z * 4 + q, c), device_id_type=MESH,
        )

    @pl.loop(0, 7)
    def _(i):
        q, c = target(i)
        multiply(q * 2 + c)
        for k in range(part):
            parcel(i, k).start()

    multiply(mine)
    kept = [pltpu.make_async_copy(cbuf.at[mine, k], place(me.q, me.c, k), ls.at[7, k]) for k in range(part)]
    for copy in kept:
        copy.start()

    @pl.loop(0, 7)
    def _(i):
        q, c = target(i)
        for k in range(part):
            mail.arrived(place(q, c, k), lr.at[q * 2 + c, k], me.partner)
            parcel(i, k).wait_send()

    for copy in kept:
        copy.wait()


def core(planes, proj, jump, cpar, rpar, dmap, imap, weights, lags, cw):
    length, rwid = jump.shape[0], rpar.shape[2]
    used, cols = cw + rwid, weights.shape[1]
    width = used + -used % 128
    fold = (rwid + 127) // 128
    f32, bf16 = jnp.float32, jnp.bfloat16
    dma, vmem = pltpu.SemaphoreType.DMA, pltpu.VMEM
    top = lags[0] + -lags[0] % 16
    part = planes // 2
    return pl.pallas_call(
        functools.partial(core_kernel, planes, lags),
        out_shape=jax.ShapeDtypeStruct((length // 8, planes * 4 * cols), bf16),
        in_specs=[VMEM] * 7,
        out_specs=ANY,
        scratch_shapes=[
            vmem((planes,) + weights.shape, bf16),
            vmem((part,) + weights.shape, bf16),
            vmem((length, 8 * width), bf16),
            vmem((8, part, length // 8, cols), bf16),
            vmem((top, proj.shape[1]), bf16),
            vmem((top + length, cw), f32),
            vmem((top + length, rwid), f32),
            vmem((length, cw), f32),
            vmem((fold, length, 128), f32),
            vmem((fold, length, 128), f32),
            vmem((rwid, 2 * fold * 128), bf16),
            vmem((length, 128), f32),
            vmem((8, 8, length), f32),
            vmem((8, 128), f32),
            vmem((planes, 8, 128), f32),
            dma((64 + 8 * planes,)), dma((4, 2)), dma((4, 2)), dma((4, 2)), dma((4, 2)), dma((planes,)), dma((part,)),
            dma((1,)), dma((8,)), dma((planes,)), dma((8, part)), dma((8, part)),
        ],
        compiler_params=pltpu.CompilerParams(
            collective_id=2, has_side_effects=True, vmem_limit_bytes=60 * 1024 * 1024
        ),
    )(proj, jump, cpar, rpar, dmap, imap, weights)


def plane_shards(
    planes,
    tokens,
    norm_gain,
    conv_val_w,
    conv_gate_w,
    rec_gate_w,
    rec_in_w,
    conv_taps,
    conv_bias,
    conv_gain,
    short_taps,
    decay_map,
    input_map,
    decay_base,
    decay_jump,
    out_conv_w,
    out_rec_w,
):
    s = lax.axis_index("sp")
    q = s % 4
    f32 = jnp.float32

    def by_mate(a):
        return a.reshape(a.shape[0], 4, a.shape[1] // 4).transpose(1, 0, 2)

    def mine(a, axis):
        size = a.shape[axis] // 4
        return lax.dynamic_slice_in_dim(a, q * size, size, axis)

    pieces = jnp.concatenate([by_mate(w) for w in (conv_val_w, conv_gate_w, rec_gate_w, rec_in_w)], axis=2)
    projected, jall = enter(planes, tokens, norm_gain[None], pieces, decay_jump)
    cw, rw = conv_val_w.shape[1] // 4, rec_in_w.shape[1] // 4
    jump = jall.reshape(-1, jall.shape[2])
    cols = out_conv_w.shape[1]
    rows_by_mate = jnp.concatenate(
        [out_conv_w.reshape(4, cw, cols), out_rec_w.reshape(4, rw, cols)], axis=1
    ).reshape(-1, cols)
    cpar = mine(jnp.concatenate([conv_taps.astype(f32), conv_bias[None], conv_gain[None]]), 1)
    rpar = by_mate(jnp.concatenate([short_taps.astype(f32), RATE_SCALE * jax.nn.softplus(-decay_base)[None]]))
    lags = (conv_taps.shape[0] - 1, short_taps.shape[0] - 1)
    return core(planes, projected, jump, cpar, rpar, decay_map, input_map, rows_by_mate, lags, cw)


def solution(mesh):
    in_specs = (
        P(("sp", "tp"), None),
        P(),
        P("sp", "tp"),
        P("sp", "tp"),
        P("sp", "tp"),
        P("sp", "tp"),
        P(None, "tp"),
        P("tp"),
        P("tp"),
        P(None, "tp"),
        P("tp", None, None),
        P("tp", None, None),
        P("tp"),
        P("sp", "tp"),
        P("tp", "sp"),
        P("tp", "sp"),
    )
    out_specs = P(("sp", "tp"), None)
    count = mesh.shape["sp"]
    planar = mesh.shape["tp"] == 2 and count % 8 == 0 and count >= 16
    body = functools.partial(plane_shards, count // 4) if planar else shards
    return jax.shard_map(body, mesh=mesh, in_specs=in_specs, out_specs=out_specs, check_vma=False)
```
